32 devices in a mesh: sp: 4 (over z), fs: 4 (over y, x), tp: 2 (over core).
Axes of the slice: x: 2, y: 2, z: 4, core: 2. Of those that a mesh axis runs over, the one named last changes fastest.
Arguments:
- tokens: bfloat16 [1024, 2048], P(('sp', 'fs', 'tp')), may hold values from -20 to 20
- norm_gain: float32 [2048], replicated, may hold values from 0.1 to 1.9
- query_weight: bfloat16 [2048, 1024], P(None, ('fs', 'tp')), may hold values from -0.5 to 0.5
- w_key: bfloat16 [2048, 256], P(None, 'tp'), may hold values from -0.5 to 0.5
- w_value: bfloat16 [2048, 256], P(None, 'tp'), may hold values from -0.125 to 0.125
- w_input: bfloat16 [2048, 1024], P(None, ('fs', 'tp')), may hold values from -0.125 to 0.125
- w_gate: bfloat16 [2048, 1024], P(None, ('fs', 'tp')), may hold values from -0.125 to 0.125
- conv_kernel: float32 [4, 1024], P(None, ('fs', 'tp')), may hold values from -3 to 3
- w_recur: bfloat16 [16, 64, 64], P(('fs', 'tp')), may hold values from -0.75 to 0.75
- w_admit: bfloat16 [16, 64, 64], P(('fs', 'tp')), may hold values from -0.75 to 0.75
- decay_param: float32 [1024], P(('fs', 'tp')), may hold values from 4 to 17
- decay_scale: float32 [1024, 1024], P('sp', ('fs', 'tp')), may hold values from 0.5 to 14336
- init_state: float32 [1024], P(('fs', 'tp')), may hold values from -6 to 6
- diff_lambda: float32 [8], P(('fs', 'tp')), may hold values from 0.3 to 0.8
- head_gain: float32 [128], replicated, may hold values from 0.1 to 1.9
- w_out_lru: bfloat16 [1024, 2048], P(('fs', 'tp')), may hold values from -1 to 1
- w_out_attn: bfloat16 [1024, 2048], P(('fs', 'tp')), may hold values from -0.1875 to 0.1875
Outputs:
- mixed: bfloat16 [1024, 2048], P(('sp', 'fs', 'tp'))
The draws below stay inside these ranges and needn't reach their ends.
All inputs are finite; a program needn't handle non-finite values.
Results may differ from the reference program's by a relative error of at most 0.019.
Values may be sent and summed in bfloat16 or wider, within the bound.
A program may use at most 64 MiB of HBM per device.

```python
import math
import jax
import jax.numpy as jnp
from jax import lax

D = 2048
W = 1024
BD = 64
BLOCKS = 16
HEADS = 8
KV_HEADS = 2
E = 64
V = 128
CONV = 4
TOK_DEV = 256
TOKEN_SPAN = 1024
N_FS = 4
N_TP = 2


def channel_rates(key):
    base = jax.random.fold_in(key, 11)
    key_pick, key_slow, key_fast = jax.random.split(base, 3)
    share = 0.5
    slow = jax.random.uniform(key_pick, (W,), jnp.float32) < share
    slow_rate = jnp.exp(jax.random.uniform(key_slow, (W,), jnp.float32, jnp.log(0.05), jnp.log(0.25))) / (4.0 * TOKEN_SPAN)
    fast_rate = jnp.exp(jax.random.uniform(key_fast, (W,), jnp.float32, jnp.log(0.01), jnp.log(0.033))) / 4.0
    return jnp.where(slow, slow_rate, fast_rate)


def draw_decay_param(key, part):
    rates = channel_rates(key)
    return jnp.clip(-jnp.log(jnp.expm1(rates)), 4.0, 17.0)


def draw_decay_scale(key, part):
    rates = channel_rates(key)
    base = jax.random.fold_in(key, 23)
    key_block, key_spot, key_loss = jax.random.split(base, 3)
    block_count = TOKEN_SPAN // TOK_DEV
    factor = jnp.exp(jax.random.uniform(key_block, (block_count, W), jnp.float32, jnp.log(0.5), jnp.log(2.0)))
    dispersed_numbers = jnp.repeat(factor, TOK_DEV, axis=0)
    spots = jax.random.randint(key_spot, (2,), 0, TOKEN_SPAN)
    losses = jax.random.uniform(key_loss, (2, W), jnp.float32, 0.2, 0.5)
    stride_displacements = -jnp.log1p(-losses) / (4.0 * rates[None, :])
    selected_members = (jnp.arange(TOKEN_SPAN)[:, None] == spots[None, :]).astype(jnp.float32)
    clustered_numbers = jnp.dot(selected_members, stride_displacements)
    masked_elements = jnp.sum(selected_members, axis=1) > 0.0
    return jnp.clip(jnp.where(masked_elements[:, None], clustered_numbers, dispersed_numbers), 0.5, 14.0 * TOKEN_SPAN)


def first_block_lean(key, values, row_scale):
    lean_key = jax.random.fold_in(key, 43)
    common = jax.random.normal(lean_key, (D,), jnp.float32)
    common = common / jnp.sqrt(jnp.sum(common * common))
    leaning = (jnp.arange(TOKEN_SPAN) < TOK_DEV)[:, None]
    blended = 0.71 * values + 0.7 * D ** 0.5 * row_scale * common[None, :]
    return jnp.where(leaning, blended, values)


def draw_tokens(key, part):
    base = jax.random.fold_in(key, 41)
    key_body, key_rows = jax.random.split(base, 2)
    row_scale = jnp.exp(jax.random.uniform(key_rows, (TOKEN_SPAN, 1), jnp.float32, jnp.log(0.3), jnp.log(3.0)))
    values = jax.random.normal(key_body, (TOKEN_SPAN, D), jnp.float32) * row_scale
    values = first_block_lean(key, values, row_scale)
    return jnp.clip(values, -20.0, 20.0).astype(jnp.bfloat16)


def draw_query_weight(key, part):
    base = jax.random.fold_in(key, 31)
    dispersed_numbers = (2.0 / D) ** 0.5
    values = jax.random.normal(base, (D, HEADS * 2 * E), jnp.float32) * dispersed_numbers
    return jnp.clip(values, -0.5, 0.5).astype(jnp.bfloat16)


def draw_w_key(key, part):
    base = jax.random.fold_in(key, 37)
    dispersed_numbers = (1.5 / D) ** 0.5
    values = jax.random.normal(base, (D, KV_HEADS * 2 * E), jnp.float32) * dispersed_numbers
    return jnp.clip(values, -0.5, 0.5).astype(jnp.bfloat16)


def block_levels(rng, dims, pieces, least, high):
    loudness = 1.0
    for axis_at, parts in pieces:
        heights = jax.random.uniform(jax.random.fold_in(jax.random.fold_in(rng, 6), axis_at), (parts,), jnp.float32, least / len(pieces), high / len(pieces))
        loudness = loudness * jnp.repeat(jnp.exp(heights), dims[axis_at] // parts).reshape((-1,) + (1,) * (len(dims) - 1 - axis_at))
    return loudness


def scatter_about(stream_key, dims, scale, most, cuts=(), kind=jnp.bfloat16):
    drawn = jax.random.normal(stream_key, dims, jnp.float32) * scale
    if len(cuts) > 0:
        drawn = block_levels(stream_key, dims, cuts, -0.22, 0.18) * drawn
    return jnp.clip(drawn, min=-most, max=most).astype(kind)


def setup_inputs(seed: int = 0) -> dict:
    arg_keys = jax.random.split(jax.random.key(seed), 18)
    return {
        "tokens": draw_tokens(jax.random.fold_in(arg_keys[17], 71), 0),
        "norm_gain": jnp.clip(1.0 + 0.18 * jax.random.normal(arg_keys[1], (D,), jnp.float32), 0.1, 1.9),
        "query_weight": draw_query_weight(jax.random.fold_in(arg_keys[17], 71), 0),
        "w_key": draw_w_key(jax.random.fold_in(arg_keys[17], 71), 0),
        "w_value": scatter_about(arg_keys[4], (D, V * KV_HEADS), D ** -0.5, 0.125, ((1, 2),)),
        "w_input": scatter_about(arg_keys[5], (D, W), D ** -0.5, 0.125, ((1, 8),)),
        "w_gate": scatter_about(arg_keys[6], (D, W), D ** -0.5, 0.125, ((1, 8),)),
        "conv_kernel": scatter_about(arg_keys[7], (CONV, W), CONV ** -0.5, 3.0, ((1, 8),), jnp.float32),
        "w_recur": scatter_about(arg_keys[8], (BLOCKS, BD, BD), BD ** -0.5, 0.75, ((0, 8),)),
        "w_admit": scatter_about(arg_keys[9], (BLOCKS, BD, BD), BD ** -0.5, 0.75, ((0, 8),)),
        "decay_param": draw_decay_param(jax.random.fold_in(arg_keys[17], 71), 0),
        "decay_scale": draw_decay_scale(jax.random.fold_in(arg_keys[17], 71), 0),
        "init_state": scatter_about(arg_keys[12], (W,), 1.0, 6.0, ((0, 8),), jnp.float32),
        "diff_lambda": jnp.clip(0.3 + 0.5 * jax.random.uniform(arg_keys[13], (HEADS,), jnp.float32) ** block_levels(arg_keys[13], (HEADS,), ((0, 8),), -0.2, 0.2), 0.3, 0.8),
        "head_gain": jnp.clip(1.0 + 0.18 * jax.random.normal(arg_keys[14], (V,), jnp.float32), 0.1, 1.9),
        "w_out_lru": scatter_about(arg_keys[15], (W, D), (W // 32) ** -0.5, 1.0, ((0, 8),)),
        "w_out_attn": scatter_about(arg_keys[16], (HEADS * V, D), (HEADS * V) ** -0.5, 0.1875, ((0, 8),)),
    }


gate_scale = 8.0
input_eps = 1e-06
head_eps = 1e-05

def pair_combine(earlier, later):
    decay_early, state_early = earlier
    decay_late, state_late = later
    return (decay_early * decay_late, decay_late * state_early + state_late)

def project(normed, weight):
    return jnp.dot(normed, weight, preferred_element_type=jnp.float32).astype(jnp.bfloat16)

def reference(tokens, norm_gain, query_weight, w_key, w_value, w_input, w_gate, conv_kernel, w_recur, w_admit, decay_param, decay_scale, init_state, diff_lambda, head_gain, w_out_lru, w_out_attn):
    floats = tokens.astype(jnp.float32)
    normed = (floats * lax.rsqrt(lax.optimization_barrier(jnp.mean(floats * floats, axis=1, keepdims=True)) + input_eps) * norm_gain).astype(jnp.bfloat16)
    query = project(normed, query_weight)
    keys_all = project(normed, w_key)
    values_all = project(normed, w_value)
    lru_in = project(normed, w_input)
    gate_proj = project(normed, w_gate)
    padded = jnp.concatenate([jnp.zeros((CONV - 1, W), jnp.bfloat16), lru_in], axis=0).astype(jnp.float32)
    conv_sum = jnp.zeros((TOKEN_SPAN, W), jnp.float32)
    for offset in range(CONV):
        conv_sum = conv_sum + conv_kernel[offset] * padded[offset:offset + TOKEN_SPAN]
    conv_out = conv_sum.astype(jnp.bfloat16)
    grouped = conv_out.astype(jnp.float32).reshape(TOKEN_SPAN, BLOCKS, BD)
    recur = jax.nn.sigmoid(jnp.einsum('tni,nij->tnj', grouped, w_recur.astype(jnp.float32)).reshape(TOKEN_SPAN, W))
    admit = jax.nn.sigmoid(jnp.einsum('tni,nij->tnj', grouped, w_admit.astype(jnp.float32)).reshape(TOKEN_SPAN, W))
    log_decay = -gate_scale * recur * jax.nn.softplus(-decay_param) * decay_scale
    decay = jnp.exp(log_decay)
    drive = jnp.sqrt(-jnp.expm1(2.0 * log_decay)) * admit * conv_out.astype(jnp.float32)
    drive = jnp.concatenate([drive[:1] + decay[:1] * init_state[None, :], drive[1:]], axis=0)
    _, states = lax.associative_scan(pair_combine, (decay, drive), axis=0)
    lru_out = (states * jax.nn.gelu(gate_proj.astype(jnp.float32))).astype(jnp.bfloat16)
    query_heads = query.reshape(TOKEN_SPAN, HEADS, 2, E).astype(jnp.float32)
    head_owner = (jnp.arange(HEADS) % KV_HEADS).astype(jnp.int32)
    key_heads = keys_all.reshape(TOKEN_SPAN, KV_HEADS, 2, E).astype(jnp.float32)[:, head_owner]
    value_heads = values_all.reshape(TOKEN_SPAN, KV_HEADS, V).astype(jnp.float32)[:, head_owner]
    query_rows = math.gcd(TOKEN_SPAN, 256)
    key_index = jnp.arange(TOKEN_SPAN).astype(jnp.int32)

    def attend_block(block_index):
        first_row = (block_index * query_rows).astype(jnp.int32)
        block = lax.dynamic_slice_in_dim(query_heads, first_row, query_rows, 0)
        scores = jnp.einsum('qhme,khme->hmqk', block, key_heads) * E ** (-0.5)
        query_index = first_row + jnp.arange(query_rows).astype(jnp.int32)
        visible = key_index[None, :] <= query_index[:, None]
        scores = jnp.where(visible, scores, -jnp.inf)
        peak = lax.optimization_barrier(jnp.max(scores, axis=-1, keepdims=True))
        expos = jnp.where(visible, jnp.exp(scores - peak), 0.0)
        total = lax.optimization_barrier(jnp.sum(expos, axis=-1))
        weights = lax.optimization_barrier(expos.astype(jnp.bfloat16)).astype(jnp.float32)
        heads_values = jnp.einsum('hmqk,khv->hmqv', weights, value_heads)
        lam = diff_lambda[:, None, None]
        diff = heads_values[:, 0] / total[:, 0, :, None] - lam * heads_values[:, 1] / total[:, 1, :, None]
        scaled = diff * lax.rsqrt(lax.optimization_barrier(jnp.mean(diff * diff, axis=-1, keepdims=True)) + head_eps) * head_gain
        return jnp.transpose(scaled, (1, 0, 2)).reshape(query_rows, HEADS * V).astype(jnp.bfloat16)
    attn_out = lax.map(attend_block, jnp.arange(TOKEN_SPAN // query_rows).astype(jnp.int32))
    attn_out = attn_out.reshape(TOKEN_SPAN, HEADS * V)
    group_count = N_FS * N_TP
    lru_cols = W // group_count
    head_cols = HEADS * V // group_count
    mixed = jnp.zeros((TOKEN_SPAN, D), jnp.float32)
    for group_index in range(group_count):
        low = group_index * lru_cols
        high = group_index * head_cols
        partial_sum = jnp.dot(lru_out[:, low:low + lru_cols], w_out_lru[low:low + lru_cols], preferred_element_type=jnp.float32)
        partial_sum = partial_sum + jnp.dot(attn_out[:, high:high + head_cols], w_out_attn[high:high + head_cols], preferred_element_type=jnp.float32)
        rounded = lax.optimization_barrier(partial_sum.astype(jnp.bfloat16))
        mixed = mixed + rounded.astype(jnp.float32)
    return mixed.astype(jnp.bfloat16)
```

```python
import functools

import jax
import jax.numpy as jnp
from jax import lax
from jax.experimental import pallas as pl
from jax.experimental.pallas import tpu as pltpu
from jax.sharding import PartitionSpec as P

gate_scale = 8.0
input_eps = 1e-06
head_eps = 1e-05
f32 = jnp.float32
bf16 = jnp.bfloat16
MESH = pl.DeviceIdType.MESH
HALO = 16


def softplus(x):
    u = jnp.exp(-jnp.abs(x))
    z = u / (2.0 + u)
    zz = z * z
    series = jnp.zeros_like(z)
    for power in range(17, 0, -2):
        series = series * zz + 1.0 / power
    return jnp.maximum(x, 0.0) + 2.0 * z * series


def neg_expm1(y, exp_y):
    series = jnp.ones_like(y)
    for k in range(8, 1, -1):
        series = 1.0 + series * y * (1.0 / k)
    return jnp.where(y > -0.25, -y * series, 1.0 - exp_y)


def shifted(x, k, fill):
    if k % 8 == 0:
        return jnp.concatenate([jnp.full((k, x.shape[1]), fill, x.dtype), x[:-k]], axis=0)
    row = lax.broadcasted_iota(jnp.int32, x.shape, 0)
    return jnp.where(row < k, fill, pltpu.roll(x, k, 0))


def kernel(
    sizes,
    tokens, norm_gain, query_weight, w_key, w_value, w_input, w_gate, conv_kernel, w_recur, w_admit,
    decay_param, decay_scale, init_state, diff_lambda, head_gain, w_out_lru, w_out_attn,
    out,
    tok, normed, w_all, w_out, conv_v, recur_v, admit_v, chan_v, scale_v, lam_v, hg_v, ng_v,
    kv, ext, halo_src, halo_dst, stat, qs, peak, total, acc, mix, send_a, recv_a, own, send_b, recv_b,
    local_sem, tok_send, tok_recv, fwd_send, fwd_recv, kv_send, kv_recv, halo_sem, stat_send, stat_recv,
    a_send, a_recv, b_send, b_recv,
):
    n_s, n_f, n_t = sizes
    s, f, t = (lax.axis_index(a) for a in ("sp", "fs", "tp"))
    group = n_f * n_t
    rows = tokens.shape[0]
    span = rows * group
    chans = w_input.shape[1]
    width = query_weight.shape[1]
    kw = w_key.shape[1]
    vw = w_value.shape[1]
    me = f * n_t + t

    here = [
        (tokens, tok.at[me]),
        (norm_gain, ng_v),
        (w_key, w_all.at[:, pl.ds(0, kw)]),
        (w_value, w_all.at[:, pl.ds(kw, vw)]),
        (w_input, w_all.at[:, pl.ds(kw + vw, chans)]),
        (w_gate, w_all.at[:, pl.ds(kw + vw + chans, chans)]),
        (query_weight, w_all.at[:, pl.ds(kw + vw + 2 * chans, width)]),
        (conv_kernel, conv_v),
        (w_recur, recur_v),
        (w_admit, admit_v),
        (decay_param, chan_v.at[0]),
        (init_state, chan_v.at[1]),
        (decay_scale, scale_v),
        (diff_lambda, lam_v),
        (head_gain, hg_v),
        (w_out_lru, w_out.at[pl.ds(0, chans)]),
        (w_out_attn, w_out.at[pl.ds(chans, w_out_attn.shape[0])]),
    ]
    here = [pltpu.make_async_copy(a, b, local_sem.at[i]) for i, (a, b) in enumerate(here)]
    for copy in here:
        copy.start()

    barrier = pltpu.get_barrier_semaphore()
    for df in range(n_f):
        for dt in range(n_t):
            if df or dt:
                pl.semaphore_signal(
                    barrier, inc=1, device_id_type=MESH,
                    device_id={"fs": lax.rem(f + df, n_f), "tp": lax.rem(t + dt, n_t)},
                )

    def greet(k, c):
        pl.semaphore_signal(barrier, inc=1, device_id={"sp": lax.rem(s + k, n_s)}, device_id_type=MESH)
        return c

    lax.fori_loop(1, n_s, greet, 0)
    pl.semaphore_wait(barrier, group - 1 + n_s - 1)

    def remote(src, dst, ss, rs, **where):
        return pltpu.make_async_remote_copy(
            src_ref=src, dst_ref=dst, send_sem=ss, recv_sem=rs, device_id=where, device_id_type=MESH
        )

    here[0].wait()
    here[1].wait()
    sends = []
    for df in range(1, n_f):
        sends.append(remote(tok.at[me], tok.at[me], tok_send.at[df], tok_recv.at[df], fs=lax.rem(f + df, n_f)))
    for copy in sends:
        copy.start()

    def forward(df):
        slot = lax.rem(f + n_f - df, n_f) * n_t + t
        for dt in range(1, n_t):
            copy = remote(
                tok.at[slot], tok.at[slot], fwd_send.at[df, dt], fwd_recv.at[df, dt], tp=lax.rem(t + dt, n_t)
            )
            copy.start()
            sends.append(copy)

    def normalize(slot):
        x = tok[slot].astype(f32)
        x = x * lax.rsqrt(jnp.mean(x * x, axis=1, keepdims=True) + input_eps) * ng_v[...]
        normed[pl.ds(pl.multiple_of(slot * rows, rows), rows), :] = x.astype(bf16)

    forward(0)
    normalize(me)
    for df in range(n_f):
        if df:
            slot = lax.rem(f + n_f - df, n_f) * n_t + t
            remote(tok.at[slot], tok.at[slot], tok_send.at[df], tok_recv.at[df], fs=f).wait_recv()
            forward(df)
            normalize(slot)
    for df in range(n_f):
        for dt in range(1, n_t):
            slot = lax.rem(f + n_f - df, n_f) * n_t + lax.rem(t + n_t - dt, n_t)
            remote(tok.at[slot], tok.at[slot], fwd_send.at[df, dt], fwd_recv.at[df, dt], tp=t).wait_recv()
            normalize(slot)

    for copy in here[2:]:
        copy.wait()
    x = normed[...]
    kv[s] = jnp.dot(x, w_all[:, : kw + vw], preferred_element_type=f32).astype(bf16)
    rest = jnp.dot(x, w_all[:, kw + vw :], preferred_element_type=f32).astype(bf16)
    lru_in = rest[:, :chans]
    halo_src[...] = lru_in[span - HALO :]

    def send_kv(k, c):
        remote(kv.at[s], kv.at[s], kv_send.at[k], kv_recv.at[s], sp=s + k).start()
        return c

    later = n_s - 1 - s
    halo_copy = remote(halo_src, halo_dst, halo_sem.at[0], halo_sem.at[1], sp=lax.rem(s + 1, n_s))

    @pl.when(s + 1 < n_s)
    def _():
        halo_copy.start()

    lax.fori_loop(1, later + 1, send_kv, 0)

    gate_proj = rest[:, chans : 2 * chans].astype(f32)
    gate = 0.5 * gate_proj * (
        1.0 + jnp.tanh(0.7978845608028654 * (gate_proj + 0.044715 * gate_proj * gate_proj * gate_proj))
    )
    q = rest[:, 2 * chans :]
    size_qk = width // 2
    first = lax.broadcasted_iota(jnp.int32, (span, width), 1) < size_qk
    zero = jnp.zeros_like(q)
    qs[pl.ds(0, span), :] = jnp.where(first, q, zero)
    qs[pl.ds(span, span), :] = jnp.where(first, zero, q)
    score_scale = size_qk ** (-0.5)

    def scores_of(j):
        return lax.dot_general(
            qs[...], kv[j, :, pl.ds(0, kw)], (((1,), (1,)), ((), ())), preferred_element_type=f32
        ) * score_scale

    ext[pl.ds(HALO, span), :] = lru_in.astype(f32)

    @pl.when(s == 0)
    def _():
        ext[pl.ds(0, HALO), :] = jnp.zeros((HALO, chans), f32)

    @pl.when(s > 0)
    def _():
        halo_copy.wait_recv()
        ext[pl.ds(0, HALO), :] = halo_dst[...].astype(f32)

    taps = conv_kernel.shape[0]
    conv = jnp.zeros((span, chans), f32)
    for j in range(taps):
        conv = conv + conv_v[pl.ds(j, 1), :] * ext[pl.ds(HALO - taps + 1 + j, span), :]
    conv = conv.astype(bf16)
    blocks, bd = w_recur.shape[0], w_recur.shape[1]
    lines = []
    for n in range(blocks):
        parts = []
        for ref in (recur_v, admit_v):
            for m in range(blocks):
                parts.append(ref[n] if m == n else jnp.zeros((bd, bd), bf16))
        lines.append(jnp.concatenate(parts, axis=1))
    gates = jax.nn.sigmoid(jnp.dot(conv, jnp.concatenate(lines, axis=0), preferred_element_type=f32))
    log_decay = -gate_scale * gates[:, :chans] * softplus(-chan_v[0]) * scale_v[...]
    a = jnp.exp(log_decay)
    b = jnp.sqrt(neg_expm1(2.0 * log_decay, a * a)) * gates[:, chans:] * conv.astype(f32)
    k = 1
    while k < span:
        b = a * shifted(b, k, 0.0) + b
        a = a * shifted(a, k, 1.0)
        k *= 2
    stat[s, pl.ds(0, 8), :] = jnp.broadcast_to(a[span - 1 :], (8, chans))
    stat[s, pl.ds(8, 8), :] = jnp.broadcast_to(b[span - 1 :], (8, chans))

    sc = scores_of(s)
    row = lax.broadcasted_iota(jnp.int32, (span, span), 0)
    col = lax.broadcasted_iota(jnp.int32, (span, span), 1)
    see = jnp.concatenate([col <= row, col <= row], axis=0)
    sc = jnp.where(see, sc, -1e30)
    top = jnp.max(sc, axis=1, keepdims=True)
    p = jnp.where(see, jnp.exp(sc - top), 0.0)

    def send_stat(k, c):
        remote(stat.at[s], stat.at[s], stat_send.at[k], stat_recv.at[s], sp=s + k).start()
        return c

    lax.fori_loop(1, later + 1, send_stat, 0)
    peak[...] = top
    total[...] = jnp.sum(p, axis=1, keepdims=True)
    acc[...] = jnp.dot(p.astype(bf16), kv[s, :, pl.ds(kw, vw)], preferred_element_type=f32)

    def enter(k, state):
        remote(stat.at[k], stat.at[k], stat_send.at[0], stat_recv.at[k], sp=s).wait_recv()
        return stat[k, pl.ds(0, 1), :] * state + stat[k, pl.ds(8, 1), :]

    entering = lax.fori_loop(0, s, enter, chan_v[1])
    lru_out = ((b + a * entering) * gate).astype(bf16)
    mix[:, :, :, pl.ds(0, chans)] = lru_out.reshape(n_f, n_t, rows, chans)

    def earlier_keys(k, c):
        j = s - 1 - k
        remote(kv.at[j], kv.at[j], kv_send.at[0], kv_recv.at[j], sp=s).wait_recv()
        sc = scores_of(j)
        old = peak[...]
        top = jnp.maximum(old, jnp.max(sc, axis=1, keepdims=True))
        p = jnp.exp(sc - top)
        fade = jnp.exp(old - top)
        peak[...] = top
        total[...] = total[...] * fade + jnp.sum(p, axis=1, keepdims=True)
        acc[...] = acc[...] * fade + jnp.dot(p.astype(bf16), kv[j, :, pl.ds(kw, vw)], preferred_element_type=f32)
        return c

    lax.fori_loop(0, s, earlier_keys, 0)
    heads = acc[...] / total[...]
    diff = heads[:span] - lam_v[...] * heads[span:]
    scaled = diff * lax.rsqrt(jnp.mean(diff * diff, axis=1, keepdims=True) + head_eps) * hg_v[...]
    mix[:, :, :, pl.ds(chans, vw)] = scaled.astype(bf16).reshape(n_f, n_t, rows, vw)

    depth = chans + vw
    for dt in range(1, n_t):
        there = lax.rem(t + dt, n_t)
        share = jnp.dot(mix[:, there].reshape(n_f * rows, depth), w_out[...], preferred_element_type=f32)
        send_a[dt - 1] = share.astype(bf16).reshape(n_f, rows, share.shape[1])
        for df in range(1, n_f + 1):
            g = lax.rem(f + df, n_f)
            copy = remote(
                send_a.at[dt - 1, g], recv_a.at[dt - 1, g], a_send.at[dt - 1, df - 1], a_recv.at[dt - 1, df - 1],
                tp=there,
            )
            copy.start()
            sends.append(copy)
    share = jnp.dot(mix[:, t].reshape(n_f * rows, depth), w_out[...], preferred_element_type=f32)
    own[...] = share.reshape(own.shape)
    for df in range(1, n_f + 1):
        g = lax.rem(f + df, n_f)
        piece = own[g]
        for dt in range(1, n_t):
            remote(
                send_a.at[dt - 1, g], recv_a.at[dt - 1, g], a_send.at[dt - 1, df - 1], a_recv.at[dt - 1, df - 1], tp=t
            ).wait_recv()
            piece = piece + recv_a[dt - 1, g].astype(f32)
        if df < n_f:
            send_b[df - 1] = piece.astype(bf16)
            copy = remote(send_b.at[df - 1], recv_b.at[df - 1], b_send.at[df - 1], b_recv.at[df - 1], fs=g)
            copy.start()
            sends.append(copy)
    for df in range(1, n_f):
        remote(send_b.at[df - 1], recv_b.at[df - 1], b_send.at[df - 1], b_recv.at[df - 1], fs=f).wait_recv()
        piece = piece + recv_b[df - 1].astype(f32)
    out[...] = piece.astype(bf16)

    for copy in sends:
        copy.wait_send()

    @pl.when(s + 1 < n_s)
    def _():
        halo_copy.wait_send()

    def drain(k, c):
        remote(kv.at[s], kv.at[s], kv_send.at[k], kv_recv.at[s], sp=s + k).wait_send()
        remote(stat.at[s], stat.at[s], stat_send.at[k], stat_recv.at[s], sp=s + k).wait_send()
        return c

    lax.fori_loop(1, later + 1, drain, 0)


def body(sizes, *args):
    n_s, n_f, n_t = sizes
    (tokens, norm_gain, query_weight, w_key, w_value, w_input, w_gate, conv_kernel, w_recur, w_admit,
     decay_param, decay_scale, init_state, diff_lambda, head_gain, w_out_lru, w_out_attn) = args
    rows, d = tokens.shape
    group = n_f * n_t
    span = rows * group
    chans = w_input.shape[1]
    kw, vw, width = w_key.shape[1], w_value.shape[1], query_weight.shape[1]
    operands = (
        tokens, norm_gain[None], query_weight, w_key, w_value, w_input, w_gate, conv_kernel, w_recur, w_admit,
        decay_param[None], decay_scale, init_state[None], diff_lambda[None], head_gain[None], w_out_lru, w_out_attn,
    )
    dma = pltpu.SemaphoreType.DMA
    scratch = [
        pltpu.VMEM((group, rows, d), bf16),
        pltpu.VMEM((span, d), bf16),
        pltpu.VMEM((d, kw + vw + 2 * chans + width), bf16),
        pltpu.VMEM((chans + vw, d), bf16),
        pltpu.VMEM(conv_kernel.shape, f32),
        pltpu.VMEM(w_recur.shape, bf16),
        pltpu.VMEM(w_admit.shape, bf16),
        pltpu.VMEM((2, 1, chans), f32),
        pltpu.VMEM((span, chans), f32),
        pltpu.VMEM((1, 1), f32),
        pltpu.VMEM((1, vw), f32),
        pltpu.VMEM((1, d), f32),
        pltpu.VMEM((n_s, span, kw + vw), bf16),
        pltpu.VMEM((span + HALO, chans), f32),
        pltpu.VMEM((HALO, chans), bf16),
        pltpu.VMEM((HALO, chans), bf16),
        pltpu.VMEM((n_s, 16, chans), f32),
        pltpu.VMEM((2 * span, width), bf16),
        pltpu.VMEM((2 * span, 1), f32),
        pltpu.VMEM((2 * span, 1), f32),
        pltpu.VMEM((2 * span, vw), f32),
        pltpu.VMEM((n_f, n_t, rows, chans + vw), bf16),
        pltpu.VMEM((n_t - 1, n_f, rows, d), bf16),
        pltpu.VMEM((n_t - 1, n_f, rows, d), bf16),
        pltpu.VMEM((n_f, rows, d), f32),
        pltpu.VMEM((n_f - 1, rows, d), bf16),
        pltpu.VMEM((n_f - 1, rows, d), bf16),
        dma((len(operands),)),
        dma((n_f,)),
        dma((n_f,)),
        dma((n_f, n_t)),
        dma((n_f, n_t)),
        dma((n_s,)),
        dma((n_s,)),
        dma((2,)),
        dma((n_s,)),
        dma((n_s,)),
        dma((n_t - 1, n_f)),
        dma((n_t - 1, n_f)),
        dma((n_f - 1,)),
        dma((n_f - 1,)),
    ]
    return pl.pallas_call(
        functools.partial(kernel, sizes),
        out_shape=jax.ShapeDtypeStruct((rows, d), bf16),
        in_specs=[pl.BlockSpec(memory_space=pl.ANY)] * len(operands),
        out_specs=pl.BlockSpec(memory_space=pltpu.VMEM),
        scratch_shapes=scratch,
        compiler_params=pltpu.CompilerParams(
            collective_id=0, has_side_effects=True, vmem_limit_bytes=48 * 1024 * 1024
        ),
    )(*operands)


def solution(mesh):
    sizes = tuple(mesh.shape[a] for a in ("sp", "fs", "tp"))
    placed = (
        P(("sp", "fs", "tp"), None),
        P(),
        P(None, ("fs", "tp")),
        P(None, "tp"),
        P(None, "tp"),
        P(None, ("fs", "tp")),
        P(None, ("fs", "tp")),
        P(None, ("fs", "tp")),
        P(("fs", "tp"), None, None),
        P(("fs", "tp"), None, None),
        P(("fs", "tp")),
        P("sp", ("fs", "tp")),
        P(("fs", "tp")),
        P(("fs", "tp")),
        P(),
        P(("fs", "tp"), None),
        P(("fs", "tp"), None),
    )
    return jax.shard_map(
        functools.partial(body, sizes), mesh=mesh, in_specs=placed, out_specs=P(("sp", "fs", "tp"), None), check_vma=False
    )
```

```python
import functools

import jax
import jax.numpy as jnp
from jax import lax
from jax.experimental import pallas as pl
from jax.experimental.pallas import tpu as pltpu
from jax.sharding import PartitionSpec as P

gate_scale = 8.0
input_eps = 1e-06
head_eps = 1e-05
f32 = jnp.float32
bf16 = jnp.bfloat16
MESH = pl.DeviceIdType.MESH
HALO = 16


def softplus(x):
    u = jnp.exp(-jnp.abs(x))
    z = u / (2.0 + u)
    zz = z * z
    series = jnp.zeros_like(z)
    for power in range(17, 0, -2):
        series = series * zz + 1.0 / power
    return jnp.maximum(x, 0.0) + 2.0 * z * series


def neg_expm1(y, exp_y):
    series = jnp.ones_like(y)
    for k in range(8, 1, -1):
        series = 1.0 + series * y * (1.0 / k)
    return jnp.where(y > -0.25, -y * series, 1.0 - exp_y)


def shifted(x, k, fill):
    if k % 8 == 0:
        return jnp.concatenate([jnp.full((k, x.shape[1]), fill, x.dtype), x[:-k]], axis=0)
    row = lax.broadcasted_iota(jnp.int32, x.shape, 0)
    return jnp.where(row < k, fill, pltpu.roll(x, k, 0))


def kernel(
    sizes,
    tokens, norm_gain, query_weight, w_key, w_value, w_input, w_gate, conv_kernel, w_recur, w_admit,
    decay_param, decay_scale, init_state, diff_lambda, head_gain, w_out_lru, w_out_attn,
    out,
    tok, normed, w_all, w_out, conv_v, recur_v, admit_v, chan_v, scale_v, hg_v, ng_v,
    kv, ext, halo_src, halo_dst, stat, qs, peak, total, acc, mix, send_a, recv_a, own, send_b, recv_b,
    local_sem, tok_send, tok_recv, fwd_send, fwd_recv, kv_send, kv_recv, halo_sem, stat_send, stat_recv,
    a_send, a_recv, b_send, b_recv,
):
    n_s, n_f, n_t = sizes
    s, f, t = (lax.axis_index(a) for a in ("sp", "fs", "tp"))
    group = n_f * n_t
    rows = tokens.shape[0]
    span = rows * group
    chans = w_input.shape[1]
    width = query_weight.shape[1]
    kw = w_key.shape[1]
    vw = w_value.shape[1]
    me = f * n_t + t

    here = [
        (tokens, tok.at[me]),
        (norm_gain, ng_v),
        (w_key, w_all.at[:, pl.ds(0, kw)]),
        (w_value, w_all.at[:, pl.ds(kw, vw)]),
        (w_input, w_all.at[:, pl.ds(kw + vw, chans)]),
        (w_gate, w_all.at[:, pl.ds(kw + vw + chans, chans)]),
        (query_weight, w_all.at[:, pl.ds(kw + vw + 2 * chans, width)]),
        (conv_kernel, conv_v),
        (w_recur, recur_v),
        (w_admit, admit_v),
        (decay_param, chan_v.at[0]),
        (init_state, chan_v.at[1]),
        (decay_scale, scale_v),
        (head_gain, hg_v),
        (w_out_lru, w_out.at[pl.ds(0, chans)]),
        (w_out_attn, w_out.at[pl.ds(chans, w_out_attn.shape[0])]),
    ]
    here = [pltpu.make_async_copy(a, b, local_sem.at[i]) for i, (a, b) in enumerate(here)]
    for copy in here:
        copy.start()

    barrier = pltpu.get_barrier_semaphore()
    for df in range(n_f):
        for dt in range(n_t):
            if df or dt:
                pl.semaphore_signal(
                    barrier, inc=1, device_id_type=MESH,
                    device_id={"fs": lax.rem(f + df, n_f), "tp": lax.rem(t + dt, n_t)},
                )

    def greet(k, c):
        pl.semaphore_signal(barrier, inc=1, device_id={"sp": lax.rem(s + k, n_s)}, device_id_type=MESH)
        return c

    lax.fori_loop(1, n_s, greet, 0)
    pl.semaphore_wait(barrier, group - 1 + n_s - 1)

    def remote(src, dst, ss, rs, **where):
        return pltpu.make_async_remote_copy(
            src_ref=src, dst_ref=dst, send_sem=ss, recv_sem=rs, device_id=where, device_id_type=MESH
        )

    here[0].wait()
    here[1].wait()
    sends = []
    for df in range(1, n_f):
        sends.append(remote(tok.at[me], tok.at[me], tok_send.at[df], tok_recv.at[df], fs=lax.rem(f + df, n_f)))
    for copy in sends:
        copy.start()

    def forward(df):
        slot = lax.rem(f + n_f - df, n_f) * n_t + t
        for dt in range(1, n_t):
            copy = remote(
                tok.at[slot], tok.at[slot], fwd_send.at[df, dt], fwd_recv.at[df, dt], tp=lax.rem(t + dt, n_t)
            )
            copy.start()
            sends.append(copy)

    def normalize(slot):
        x = tok[slot].astype(f32)
        x = x * lax.rsqrt(jnp.mean(x * x, axis=1, keepdims=True) + input_eps) * ng_v[...]
        normed[pl.ds(pl.multiple_of(slot * rows, rows), rows), :] = x.astype(bf16)

    forward(0)
    normalize(me)
    for df in range(n_f):
        if df:
            slot = lax.rem(f + n_f - df, n_f) * n_t + t
            remote(tok.at[slot], tok.at[slot], tok_send.at[df], tok_recv.at[df], fs=f).wait_recv()
            forward(df)
            normalize(slot)
    for df in range(n_f):
        for dt in range(1, n_t):
            slot = lax.rem(f + n_f - df, n_f) * n_t + lax.rem(t + n_t - dt, n_t)
            remote(tok.at[slot], tok.at[slot], fwd_send.at[df, dt], fwd_recv.at[df, dt], tp=t).wait_recv()
            normalize(slot)

    for copy in here[2:]:
        copy.wait()
    x = normed[...]
    kv[s] = jnp.dot(x, w_all[:, : kw + vw], preferred_element_type=f32).astype(bf16)
    rest = jnp.dot(x, w_all[:, kw + vw :], preferred_element_type=f32).astype(bf16)
    lru_in = rest[:, :chans]
    halo_src[...] = lru_in[span - HALO :]

    def send_kv(k, c):
        remote(kv.at[s], kv.at[s], kv_send.at[k], kv_recv.at[s], sp=s + k).start()
        return c

    later = n_s - 1 - s
    halo_copy = remote(halo_src, halo_dst, halo_sem.at[0], halo_sem.at[1], sp=lax.rem(s + 1, n_s))

    @pl.when(s + 1 < n_s)
    def _():
        halo_copy.start()

    lax.fori_loop(1, later + 1, send_kv, 0)

    gate_proj = rest[:, chans : 2 * chans].astype(f32)
    gate = 0.5 * gate_proj * (
        1.0 + jnp.tanh(0.7978845608028654 * (gate_proj + 0.044715 * gate_proj * gate_proj * gate_proj))
    )
    q = rest[:, 2 * chans :]
    size_qk = width // 2
    first = lax.broadcasted_iota(jnp.int32, (span, width), 1) < size_qk
    zero = jnp.zeros_like(q)
    qs[pl.ds(0, span), :] = jnp.where(first, q, zero)
    qs[pl.ds(span, span), :] = jnp.where(first, zero, q)
    score_scale = size_qk ** (-0.5)

    def scores_of(j):
        return lax.dot_general(
            qs[...], kv[j, :, pl.ds(0, kw)], (((1,), (1,)), ((), ())), preferred_element_type=f32
        ) * score_scale

    ext[pl.ds(HALO, span), :] = lru_in.astype(f32)

    @pl.when(s == 0)
    def _():
        ext[pl.ds(0, HALO), :] = jnp.zeros((HALO, chans), f32)

    @pl.when(s > 0)
    def _():
        halo_copy.wait_recv()
        ext[pl.ds(0, HALO), :] = halo_dst[...].astype(f32)

    taps = conv_kernel.shape[0]
    conv = jnp.zeros((span, chans), f32)
    for j in range(taps):
        conv = conv + conv_v[pl.ds(j, 1), :] * ext[pl.ds(HALO - taps + 1 + j, span), :]
    conv = conv.astype(bf16)
    blocks, bd = w_recur.shape[0], w_recur.shape[1]
    lines = []
    for n in range(blocks):
        parts = []
        for ref in (recur_v, admit_v):
            for m in range(blocks):
                parts.append(ref[n] if m == n else jnp.zeros((bd, bd), bf16))
        lines.append(jnp.concatenate(parts, axis=1))
    gates = jax.nn.sigmoid(jnp.dot(conv, jnp.concatenate(lines, axis=0), preferred_element_type=f32))
    log_decay = -gate_scale * gates[:, :chans] * softplus(-chan_v[0]) * scale_v[...]
    a = jnp.exp(log_decay)
    b = jnp.sqrt(neg_expm1(2.0 * log_decay, a * a)) * gates[:, chans:] * conv.astype(f32)
    k = 1
    while k < span:
        b = a * shifted(b, k, 0.0) + b
        a = a * shifted(a, k, 1.0)
        k *= 2
    stat[s, pl.ds(0, 8), :] = jnp.broadcast_to(a[span - 1 :], (8, chans))
    stat[s, pl.ds(8, 8), :] = jnp.broadcast_to(b[span - 1 :], (8, chans))

    sc = scores_of(s)
    row = lax.broadcasted_iota(jnp.int32, (span, span), 0)
    col = lax.broadcasted_iota(jnp.int32, (span, span), 1)
    see = jnp.concatenate([col <= row, col <= row], axis=0)
    sc = jnp.where(see, sc, -1e30)
    top = jnp.max(sc, axis=1, keepdims=True)
    p = jnp.where(see, jnp.exp(sc - top), 0.0)

    def send_stat(k, c):
        remote(stat.at[s], stat.at[s], stat_send.at[k], stat_recv.at[s], sp=s + k).start()
        return c

    lax.fori_loop(1, later + 1, send_stat, 0)
    peak[...] = top
    total[...] = jnp.sum(p, axis=1, keepdims=True)
    acc[...] = jnp.dot(p.astype(bf16), kv[s, :, pl.ds(kw, vw)], preferred_element_type=f32)

    def enter(k, state):
        remote(stat.at[k], stat.at[k], stat_send.at[0], stat_recv.at[k], sp=s).wait_recv()
        return stat[k, pl.ds(0, 1), :] * state + stat[k, pl.ds(8, 1), :]

    entering = lax.fori_loop(0, s, enter, chan_v[1])
    lru_out = ((b + a * entering) * gate).astype(bf16)
    mix[:, :, :, pl.ds(0, chans)] = lru_out.reshape(n_f, n_t, rows, chans)

    def earlier_keys(k, c):
        j = s - 1 - k
        remote(kv.at[j], kv.at[j], kv_send.at[0], kv_recv.at[j], sp=s).wait_recv()
        sc = scores_of(j)
        old = peak[...]
        top = jnp.maximum(old, jnp.max(sc, axis=1, keepdims=True))
        p = jnp.exp(sc - top)
        fade = jnp.exp(old - top)
        peak[...] = top
        total[...] = total[...] * fade + jnp.sum(p, axis=1, keepdims=True)
        acc[...] = acc[...] * fade + jnp.dot(p.astype(bf16), kv[j, :, pl.ds(kw, vw)], preferred_element_type=f32)
        return c

    lax.fori_loop(0, s, earlier_keys, 0)
    heads = acc[...] / total[...]
    diff = heads[:span] - diff_lambda[0] * heads[span:]
    scaled = diff * lax.rsqrt(jnp.mean(diff * diff, axis=1, keepdims=True) + head_eps) * hg_v[...]
    mix[:, :, :, pl.ds(chans, vw)] = scaled.astype(bf16).reshape(n_f, n_t, rows, vw)

    depth = chans + vw
    for dt in range(1, n_t):
        there = lax.rem(t + dt, n_t)
        share = jnp.dot(mix[:, there].reshape(n_f * rows, depth), w_out[...], preferred_element_type=f32)
        send_a[dt - 1] = share.astype(bf16).reshape(n_f, rows, share.shape[1])
        for df in range(1, n_f + 1):
            g = lax.rem(f + df, n_f)
            copy = remote(
                send_a.at[dt - 1, g], recv_a.at[dt - 1, g], a_send.at[dt - 1, df - 1], a_recv.at[dt - 1, df - 1],
                tp=there,
            )
            copy.start()
            sends.append(copy)
    share = jnp.dot(mix[:, t].reshape(n_f * rows, depth), w_out[...], preferred_element_type=f32)
    own[...] = share.reshape(own.shape)
    for df in range(1, n_f + 1):
        g = lax.rem(f + df, n_f)
        piece = own[g]
        for dt in range(1, n_t):
            remote(
                send_a.at[dt - 1, g], recv_a.at[dt - 1, g], a_send.at[dt - 1, df - 1], a_recv.at[dt - 1, df - 1], tp=t
            ).wait_recv()
            piece = piece + recv_a[dt - 1, g].astype(f32)
        if df < n_f:
            send_b[df - 1] = piece.astype(bf16)
            copy = remote(send_b.at[df - 1], recv_b.at[df - 1], b_send.at[df - 1], b_recv.at[df - 1], fs=g)
            copy.start()
            sends.append(copy)
    for df in range(1, n_f):
        remote(send_b.at[df - 1], recv_b.at[df - 1], b_send.at[df - 1], b_recv.at[df - 1], fs=f).wait_recv()
        piece = piece + recv_b[df - 1].astype(f32)
    out[...] = piece.astype(bf16)

    for copy in sends:
        copy.wait_send()

    @pl.when(s + 1 < n_s)
    def _():
        halo_copy.wait_send()

    def drain(k, c):
        remote(kv.at[s], kv.at[s], kv_send.at[k], kv_recv.at[s], sp=s + k).wait_send()
        remote(stat.at[s], stat.at[s], stat_send.at[k], stat_recv.at[s], sp=s + k).wait_send()
        return c

    lax.fori_loop(1, later + 1, drain, 0)


def body(sizes, *args):
    n_s, n_f, n_t = sizes
    (tokens, norm_gain, query_weight, w_key, w_value, w_input, w_gate, conv_kernel, w_recur, w_admit,
     decay_param, decay_scale, init_state, diff_lambda, head_gain, w_out_lru, w_out_attn) = args
    rows, d = tokens.shape
    group = n_f * n_t
    span = rows * group
    chans = w_input.shape[1]
    kw, vw, width = w_key.shape[1], w_value.shape[1], query_weight.shape[1]
    operands = (
        tokens, norm_gain[None], query_weight, w_key, w_value, w_input, w_gate, conv_kernel, w_recur, w_admit,
        decay_param[None], decay_scale, init_state[None], diff_lambda, head_gain[None], w_out_lru, w_out_attn,
    )
    dma = pltpu.SemaphoreType.DMA
    scratch = [
        pltpu.VMEM((group, rows, d), bf16),
        pltpu.VMEM((span, d), bf16),
        pltpu.VMEM((d, kw + vw + 2 * chans + width), bf16),
        pltpu.VMEM((chans + vw, d), bf16),
        pltpu.VMEM(conv_kernel.shape, f32),
        pltpu.VMEM(w_recur.shape, bf16),
        pltpu.VMEM(w_admit.shape, bf16),
        pltpu.VMEM((2, 1, chans), f32),
        pltpu.VMEM((span, chans), f32),
        pltpu.VMEM((1, vw), f32),
        pltpu.VMEM((1, d), f32),
        pltpu.VMEM((n_s, span, kw + vw), bf16),
        pltpu.VMEM((span + HALO, chans), f32),
        pltpu.VMEM((HALO, chans), bf16),
        pltpu.VMEM((HALO, chans), bf16),
        pltpu.VMEM((n_s, 16, chans), f32),
        pltpu.VMEM((2 * span, width), bf16),
        pltpu.VMEM((2 * span, 1), f32),
        pltpu.VMEM((2 * span, 1), f32),
        pltpu.VMEM((2 * span, vw), f32),
        pltpu.VMEM((n_f, n_t, rows, chans + vw), bf16),
        pltpu.VMEM((n_t - 1, n_f, rows, d), bf16),
        pltpu.VMEM((n_t - 1, n_f, rows, d), bf16),
        pltpu.VMEM((n_f, rows, d), f32),
        pltpu.VMEM((n_f - 1, rows, d), bf16),
        pltpu.VMEM((n_f - 1, rows, d), bf16),
        dma((len(operands),)),
        dma((n_f,)),
        dma((n_f,)),
        dma((n_f, n_t)),
        dma((n_f, n_t)),
        dma((n_s,)),
        dma((n_s,)),
        dma((2,)),
        dma((n_s,)),
        dma((n_s,)),
        dma((n_t - 1, n_f)),
        dma((n_t - 1, n_f)),
        dma((n_f - 1,)),
        dma((n_f - 1,)),
    ]
    return pl.pallas_call(
        functools.partial(kernel, sizes),
        out_shape=jax.ShapeDtypeStruct((rows, d), bf16),
        in_specs=[pl.BlockSpec(memory_space=pltpu.SMEM if a is diff_lambda else pl.ANY) for a in operands],
        out_specs=pl.BlockSpec(memory_space=pltpu.VMEM),
        scratch_shapes=scratch,
        compiler_params=pltpu.CompilerParams(
            collective_id=0, has_side_effects=True, vmem_limit_bytes=67043328
        ),
    )(*operands)


def solution(mesh):
    sizes = tuple(mesh.shape[a] for a in ("sp", "fs", "tp"))
    placed = (
        P(("sp", "fs", "tp"), None),
        P(),
        P(None, ("fs", "tp")),
        P(None, "tp"),
        P(None, "tp"),
        P(None, ("fs", "tp")),
        P(None, ("fs", "tp")),
        P(None, ("fs", "tp")),
        P(("fs", "tp"), None, None),
        P(("fs", "tp"), None, None),
        P(("fs", "tp")),
        P("sp", ("fs", "tp")),
        P(("fs", "tp")),
        P(("fs", "tp")),
        P(),
        P(("fs", "tp"), None),
        P(("fs", "tp"), None),
    )
    return jax.shard_map(
        functools.partial(body, sizes), mesh=mesh, in_specs=placed, out_specs=P(("sp", "fs", "tp"), None), check_vma=False
    )
```

```python
import functools

import jax
import jax.numpy as jnp
from jax import lax
from jax.experimental import pallas as pl
from jax.experimental.pallas import tpu as pltpu
from jax.sharding import PartitionSpec as P

gate_scale = 8.0
input_eps = 1e-06
head_eps = 1e-05
f32 = jnp.float32
bf16 = jnp.bfloat16
MESH = pl.DeviceIdType.MESH
HALO = 16


def softplus(x):
    u = jnp.exp(-jnp.abs(x))
    z = u / (2.0 + u)
    zz = z * z
    series = jnp.zeros_like(z)
    for power in range(17, 0, -2):
        series = series * zz + 1.0 / power
    return jnp.maximum(x, 0.0) + 2.0 * z * series


def neg_expm1(y, exp_y):
    series = jnp.ones_like(y)
    for k in range(8, 1, -1):
        series = 1.0 + series * y * (1.0 / k)
    return jnp.where(y > -0.25, -y * series, 1.0 - exp_y)


def shifted(x, k, fill):
    if k % 8 == 0:
        return jnp.concatenate([jnp.full((k, x.shape[1]), fill, x.dtype), x[:-k]], axis=0)
    row = lax.broadcasted_iota(jnp.int32, x.shape, 0)
    return jnp.where(row < k, fill, pltpu.roll(x, k, 0))


def kernel(
    sizes,
    tokens, norm_gain, query_weight, w_key, w_value, w_input, w_gate, conv_kernel, w_recur, w_admit,
    decay_param, decay_scale, init_state, diff_lambda, head_gain, w_out_lru, w_out_attn,
    out,
    tok, normed, w_all, w_out, conv_v, recur_v, admit_v, chan_v, scale_v, hg_v, ng_v,
    kv, ext, halo_src, halo_dst, stat, qs, peak, total, acc, mix, send_a, recv_a, own, send_b, recv_b,
    local_sem, tok_send, tok_recv, fwd_send, fwd_recv, kv_send, kv_recv, halo_sem, stat_send, stat_recv,
    a_send, a_recv, b_send, b_recv, near_send, near_recv,
):
    n_s, n_f, n_t = sizes
    assert n_f == 4
    s, f, t = (lax.axis_index(a) for a in ("sp", "fs", "tp"))
    group = n_f * n_t
    rows = tokens.shape[0]
    span = rows * group
    chans = w_input.shape[1]
    width = query_weight.shape[1]
    kw = w_key.shape[1]
    vw = w_value.shape[1]
    me = f * n_t + t

    here = [
        (tokens, tok.at[me]),
        (norm_gain, ng_v),
        (w_key, w_all.at[:, pl.ds(0, kw)]),
        (w_value, w_all.at[:, pl.ds(kw, vw)]),
        (w_input, w_all.at[:, pl.ds(kw + vw, chans)]),
        (w_gate, w_all.at[:, pl.ds(kw + vw + chans, chans)]),
        (query_weight, w_all.at[:, pl.ds(kw + vw + 2 * chans, width)]),
        (conv_kernel, conv_v),
        (w_recur, recur_v),
        (w_admit, admit_v),
        (decay_param, chan_v.at[0]),
        (init_state, chan_v.at[1]),
        (decay_scale, scale_v),
        (head_gain, hg_v),
        (w_out_lru, w_out.at[pl.ds(0, chans)]),
        (w_out_attn, w_out.at[pl.ds(chans, w_out_attn.shape[0])]),
    ]
    here = [pltpu.make_async_copy(a, b, local_sem.at[i]) for i, (a, b) in enumerate(here)]
    for copy in here:
        copy.start()

    barrier = pltpu.get_barrier_semaphore()
    for df in range(n_f):
        for dt in range(n_t):
            if df or dt:
                pl.semaphore_signal(
                    barrier, inc=1, device_id_type=MESH,
                    device_id={"fs": lax.rem(f + df, n_f), "tp": lax.rem(t + dt, n_t)},
                )

    def greet(k, c):
        pl.semaphore_signal(barrier, inc=1, device_id={"sp": lax.rem(s + k, n_s)}, device_id_type=MESH)
        return c

    lax.fori_loop(1, n_s, greet, 0)
    pl.semaphore_wait(barrier, group - 1 + n_s - 1)

    def remote(src, dst, ss, rs, **where):
        return pltpu.make_async_remote_copy(
            src_ref=src, dst_ref=dst, send_sem=ss, recv_sem=rs, device_id=where, device_id_type=MESH
        )

    here[0].wait()
    here[1].wait()
    sends = []
    half = rows // 2
    near = f + 1 - 2 * lax.rem(f, 2)
    far = lax.rem(f + n_f // 2, n_f)
    diagonal = lax.rem(near + n_f // 2, n_f)

    def part(owner, core, h):
        return tok.at[owner * n_t + core, pl.ds(h * half, half)]

    def gather(owner, h, slot, target):
        copy = remote(part(owner, t, h), part(owner, t, h), tok_send.at[slot], tok_recv.at[slot], fs=target)
        copy.start()
        sends.append(copy)

    gather(f, 0, 0, near)
    gather(f, 1, 3, far)
    gather(f, 1, 1, near)
    gather(f, 0, 2, far)

    def arrived(owner, h, slot):
        remote(part(owner, t, h), part(owner, t, h), tok_send.at[slot], tok_recv.at[slot], fs=f).wait_recv()
        if slot == 0:
            gather(owner, h, 4, far)
        if slot == 3:
            gather(owner, h, 5, near)
        forward(owner, h, slot)

    def forward(owner, h, slot):
        for dt in range(1, n_t):
            copy = remote(
                part(owner, t, h), part(owner, t, h), fwd_send.at[slot, dt], fwd_recv.at[slot, dt],
                tp=lax.rem(t + dt, n_t),
            )
            copy.start()
            sends.append(copy)

    def partner(owner, first_slot):
        for dt in range(1, n_t):
            core = lax.rem(t + n_t - dt, n_t)
            for h in range(2):
                slot = first_slot + h
                remote(
                    part(owner, core, h), part(owner, core, h), fwd_send.at[slot, dt], fwd_recv.at[slot, dt], tp=t
                ).wait_recv()
            normalize(owner * n_t + core)

    def normalize(slot):
        x = tok[slot].astype(f32)
        x = x * lax.rsqrt(jnp.mean(x * x, axis=1, keepdims=True) + input_eps) * ng_v[...]
        normed[pl.ds(pl.multiple_of(slot * rows, rows), rows), :] = x.astype(bf16)

    forward(f, 0, 6)
    forward(f, 1, 7)
    normalize(me)
    partner(f, 6)
    arrived(near, 0, 0)
    arrived(far, 1, 3)
    arrived(near, 1, 1)
    arrived(far, 0, 2)
    normalize(near * n_t + t)
    normalize(far * n_t + t)
    partner(near, 0)
    partner(far, 2)
    arrived(diagonal, 0, 4)
    arrived(diagonal, 1, 5)
    normalize(diagonal * n_t + t)
    partner(diagonal, 4)

    for copy in here[2:]:
        copy.wait()
    x = normed[...]
    kv[s] = jnp.dot(x, w_all[:, : kw + vw], preferred_element_type=f32).astype(bf16)
    piece_rows = span // n_f
    mine = pl.ds(pl.multiple_of(f * piece_rows, piece_rows), piece_rows)

    def send_kv(k, c):
        remote(kv.at[s, mine], kv.at[s, mine], kv_send.at[k], kv_recv.at[s], sp=s + k).start()
        return c

    later = n_s - 1 - s
    rest = jnp.dot(x, w_all[:, kw + vw :], preferred_element_type=f32).astype(bf16)
    lru_in = rest[:, :chans]
    halo_src[...] = lru_in[span - HALO :]
    lax.fori_loop(1, later + 1, send_kv, 0)
    halo_copy = remote(halo_src, halo_dst, halo_sem.at[0], halo_sem.at[1], sp=lax.rem(s + 1, n_s))

    @pl.when(s + 1 < n_s)
    def _():
        halo_copy.start()

    gate_proj = rest[:, chans : 2 * chans].astype(f32)
    gate = 0.5 * gate_proj * (
        1.0 + jnp.tanh(0.7978845608028654 * (gate_proj + 0.044715 * gate_proj * gate_proj * gate_proj))
    )
    q = rest[:, 2 * chans :]
    size_qk = width // 2
    first = lax.broadcasted_iota(jnp.int32, (span, width), 1) < size_qk
    zero = jnp.zeros_like(q)
    qs[pl.ds(0, span), :] = jnp.where(first, q, zero)
    qs[pl.ds(span, span), :] = jnp.where(first, zero, q)
    score_scale = size_qk ** (-0.5)

    def scores_of(j):
        return lax.dot_general(
            qs[...], kv[j, :, pl.ds(0, kw)], (((1,), (1,)), ((), ())), preferred_element_type=f32
        ) * score_scale

    ext[pl.ds(HALO, span), :] = lru_in.astype(f32)

    @pl.when(s == 0)
    def _():
        ext[pl.ds(0, HALO), :] = jnp.zeros((HALO, chans), f32)

    @pl.when(s > 0)
    def _():
        halo_copy.wait_recv()
        ext[pl.ds(0, HALO), :] = halo_dst[...].astype(f32)

    taps = conv_kernel.shape[0]
    conv = jnp.zeros((span, chans), f32)
    for j in range(taps):
        conv = conv + conv_v[pl.ds(j, 1), :] * ext[pl.ds(HALO - taps + 1 + j, span), :]
    conv = conv.astype(bf16)
    blocks, bd = w_recur.shape[0], w_recur.shape[1]
    lines = []
    for n in range(blocks):
        parts = []
        for ref in (recur_v, admit_v):
            for m in range(blocks):
                parts.append(ref[n] if m == n else jnp.zeros((bd, bd), bf16))
        lines.append(jnp.concatenate(parts, axis=1))
    gates = jax.nn.sigmoid(jnp.dot(conv, jnp.concatenate(lines, axis=0), preferred_element_type=f32))
    log_decay = -gate_scale * gates[:, :chans] * softplus(-chan_v[0]) * scale_v[...]
    a = jnp.exp(log_decay)
    b = jnp.sqrt(neg_expm1(2.0 * log_decay, a * a)) * gates[:, chans:] * conv.astype(f32)
    k = 1
    while k < span:
        b = a * shifted(b, k, 0.0) + b
        a = a * shifted(a, k, 1.0)
        k *= 2
    stat[s, pl.ds(0, 8), :] = jnp.broadcast_to(a[span - 1 :], (8, chans))
    stat[s, pl.ds(8, 8), :] = jnp.broadcast_to(b[span - 1 :], (8, chans))

    def send_stat(k, c):
        remote(stat.at[s], stat.at[s], stat_send.at[k], stat_recv.at[s], sp=s + k).start()
        return c

    lax.fori_loop(1, later + 1, send_stat, 0)

    def spread(df, j):
        return remote(
            kv.at[j, mine], kv.at[j, mine], near_send.at[j, df], near_recv.at[j, df], fs=lax.rem(f + df, n_f)
        )

    def pass_on(k, c):
        j = s - 1 - k
        remote(kv.at[j, mine], kv.at[j, mine], kv_send.at[0], kv_recv.at[j], sp=s).wait_recv()
        for df in range(1, n_f):
            spread(df, j).start()
        return c

    lax.fori_loop(0, jnp.minimum(s, 1), pass_on, 0)

    sc = scores_of(s)
    row = lax.broadcasted_iota(jnp.int32, (span, span), 0)
    col = lax.broadcasted_iota(jnp.int32, (span, span), 1)
    see = jnp.concatenate([col <= row, col <= row], axis=0)
    sc = jnp.where(see, sc, -1e30)
    top = jnp.max(sc, axis=1, keepdims=True)
    p = jnp.where(see, jnp.exp(sc - top), 0.0)

    peak[...] = top
    total[...] = jnp.sum(p, axis=1, keepdims=True)
    acc[...] = jnp.dot(p.astype(bf16), kv[s, :, pl.ds(kw, vw)], preferred_element_type=f32)

    lax.fori_loop(1, s, pass_on, 0)

    def earlier_keys(k, c):
        j = s - 1 - k
        for df in range(1, n_f):
            theirs = lax.rem(f + n_f - df, n_f) * piece_rows
            theirs = pl.ds(pl.multiple_of(theirs, piece_rows), piece_rows)
            remote(kv.at[j, theirs], kv.at[j, theirs], near_send.at[j, df], near_recv.at[j, df], fs=f).wait_recv()
        sc = scores_of(j)
        old = peak[...]
        top = jnp.maximum(old, jnp.max(sc, axis=1, keepdims=True))
        p = jnp.exp(sc - top)
        fade = jnp.exp(old - top)
        peak[...] = top
        total[...] = total[...] * fade + jnp.sum(p, axis=1, keepdims=True)
        acc[...] = acc[...] * fade + jnp.dot(p.astype(bf16), kv[j, :, pl.ds(kw, vw)], preferred_element_type=f32)
        return c

    lax.fori_loop(0, s, earlier_keys, 0)
    def enter(k, state):
        remote(stat.at[k], stat.at[k], stat_send.at[0], stat_recv.at[k], sp=s).wait_recv()
        return stat[k, pl.ds(0, 1), :] * state + stat[k, pl.ds(8, 1), :]

    entering = lax.fori_loop(0, s, enter, chan_v[1])
    lru_out = ((b + a * entering) * gate).astype(bf16)
    mix[:, :, :, pl.ds(0, chans)] = lru_out.reshape(n_f, n_t, rows, chans)

    heads = acc[...] / total[...]
    diff = heads[:span] - diff_lambda[0] * heads[span:]
    scaled = diff * lax.rsqrt(jnp.mean(diff * diff, axis=1, keepdims=True) + head_eps) * hg_v[...]
    mix[:, :, :, pl.ds(chans, vw)] = scaled.astype(bf16).reshape(n_f, n_t, rows, vw)

    depth = chans + vw
    order = (diagonal, near, far, f)
    cut = out.shape[1] // 2

    def reduce(slot, target, value):
        send_b[slot] = value.astype(bf16)
        copy = remote(send_b.at[slot], recv_b.at[slot], b_send.at[slot], b_recv.at[slot], fs=target)
        copy.start()
        sends.append(copy)

    def taken(slot):
        remote(send_b.at[slot], recv_b.at[slot], b_send.at[slot], b_recv.at[slot], fs=f).wait_recv()
        return recv_b[slot].astype(f32)

    for dt in range(1, n_t):
        there = lax.rem(t + dt, n_t)
        share = jnp.dot(mix[:, there].reshape(n_f * rows, depth), w_out[...], preferred_element_type=f32)
        send_a[dt - 1] = share.astype(bf16).reshape(n_f, rows, share.shape[1])
        for i, g in enumerate(order):
            copy = remote(
                send_a.at[dt - 1, g], recv_a.at[dt - 1, g], a_send.at[dt - 1, i], a_recv.at[dt - 1, i], tp=there
            )
            copy.start()
            sends.append(copy)
    share = jnp.dot(mix[:, t].reshape(n_f * rows, depth), w_out[...], preferred_element_type=f32)
    own[...] = share.reshape(own.shape)
    for i, g in enumerate(order):
        for dt in range(1, n_t):
            remote(
                send_a.at[dt - 1, g], recv_a.at[dt - 1, g], a_send.at[dt - 1, i], a_recv.at[dt - 1, i], tp=t
            ).wait_recv()
            own[g] += recv_a[dt - 1, g].astype(f32)
        if g is diagonal:
            reduce(0, near, own[g, :, :cut])
            reduce(1, far, own[g, :, cut:])
        if g is near:
            reduce(2, near, own[g, :, :cut])
        if g is far:
            reduce(3, far, own[g, :, cut:])
    reduce(4, far, own[far, :, :cut] + taken(0))
    reduce(5, near, own[near, :, cut:] + taken(1))
    left = own[f, :, :cut] + taken(2)
    right = own[f, :, cut:] + taken(3)
    out[:, :cut] = (left + taken(4)).astype(bf16)
    out[:, cut:] = (right + taken(5)).astype(bf16)

    for copy in sends:
        copy.wait_send()

    @pl.when(s + 1 < n_s)
    def _():
        halo_copy.wait_send()

    def drain(k, c):
        remote(kv.at[s, mine], kv.at[s, mine], kv_send.at[k], kv_recv.at[s], sp=s + k).wait_send()
        remote(stat.at[s], stat.at[s], stat_send.at[k], stat_recv.at[s], sp=s + k).wait_send()
        return c

    lax.fori_loop(1, later + 1, drain, 0)

    def drain_near(j, c):
        for df in range(1, n_f):
            spread(df, j).wait_send()
        return c

    lax.fori_loop(0, s, drain_near, 0)


def body(sizes, *args):
    n_s, n_f, n_t = sizes
    (tokens, norm_gain, query_weight, w_key, w_value, w_input, w_gate, conv_kernel, w_recur, w_admit,
     decay_param, decay_scale, init_state, diff_lambda, head_gain, w_out_lru, w_out_attn) = args
    rows, d = tokens.shape
    group = n_f * n_t
    span = rows * group
    chans = w_input.shape[1]
    kw, vw, width = w_key.shape[1], w_value.shape[1], query_weight.shape[1]
    operands = (
        tokens, norm_gain[None], query_weight, w_key, w_value, w_input, w_gate, conv_kernel, w_recur, w_admit,
        decay_param[None], decay_scale, init_state[None], diff_lambda, head_gain[None], w_out_lru, w_out_attn,
    )
    dma = pltpu.SemaphoreType.DMA
    scratch = [
        pltpu.VMEM((group, rows, d), bf16),
        pltpu.VMEM((span, d), bf16),
        pltpu.VMEM((d, kw + vw + 2 * chans + width), bf16),
        pltpu.VMEM((chans + vw, d), bf16),
        pltpu.VMEM(conv_kernel.shape, f32),
        pltpu.VMEM(w_recur.shape, bf16),
        pltpu.VMEM(w_admit.shape, bf16),
        pltpu.VMEM((2, 1, chans), f32),
        pltpu.VMEM((span, chans), f32),
        pltpu.VMEM((1, vw), f32),
        pltpu.VMEM((1, d), f32),
        pltpu.VMEM((n_s, span, kw + vw), bf16),
        pltpu.VMEM((span + HALO, chans), f32),
        pltpu.VMEM((HALO, chans), bf16),
        pltpu.VMEM((HALO, chans), bf16),
        pltpu.VMEM((n_s, 16, chans), f32),
        pltpu.VMEM((2 * span, width), bf16),
        pltpu.VMEM((2 * span, 1), f32),
        pltpu.VMEM((2 * span, 1), f32),
        pltpu.VMEM((2 * span, vw), f32),
        pltpu.VMEM((n_f, n_t, rows, chans + vw), bf16),
        pltpu.VMEM((n_t - 1, n_f, rows, d), bf16),
        pltpu.VMEM((n_t - 1, n_f, rows, d), bf16),
        pltpu.VMEM((n_f, rows, d), f32),
        pltpu.VMEM((6, rows, d // 2), bf16),
        pltpu.VMEM((6, rows, d // 2), bf16),
        dma((len(operands),)),
        dma((6,)),
        dma((6,)),
        dma((8, n_t)),
        dma((8, n_t)),
        dma((n_s,)),
        dma((n_s,)),
        dma((2,)),
        dma((n_s,)),
        dma((n_s,)),
        dma((n_t - 1, n_f)),
        dma((n_t - 1, n_f)),
        dma((6,)),
        dma((6,)),
        dma((n_s, n_f)),
        dma((n_s, n_f)),
    ]
    return pl.pallas_call(
        functools.partial(kernel, sizes),
        out_shape=jax.ShapeDtypeStruct((rows, d), bf16),
        in_specs=[pl.BlockSpec(memory_space=pltpu.SMEM if a is diff_lambda else pl.ANY) for a in operands],
        out_specs=pl.BlockSpec(memory_space=pltpu.VMEM),
        scratch_shapes=scratch,
        compiler_params=pltpu.CompilerParams(
            collective_id=0, has_side_effects=True, vmem_limit_bytes=67043328
        ),
    )(*operands)


def solution(mesh):
    sizes = tuple(mesh.shape[a] for a in ("sp", "fs", "tp"))
    placed = (
        P(("sp", "fs", "tp"), None),
        P(),
        P(None, ("fs", "tp")),
        P(None, "tp"),
        P(None, "tp"),
        P(None, ("fs", "tp")),
        P(None, ("fs", "tp")),
        P(None, ("fs", "tp")),
        P(("fs", "tp"), None, None),
        P(("fs", "tp"), None, None),
        P(("fs", "tp")),
        P("sp", ("fs", "tp")),
        P(("fs", "tp")),
        P(("fs", "tp")),
        P(),
        P(("fs", "tp"), None),
        P(("fs", "tp"), None),
    )
    return jax.shard_map(
        functools.partial(body, sizes), mesh=mesh, in_specs=placed, out_specs=P(("sp", "fs", "tp"), None), check_vma=False
    )
```

```python
import functools

import jax
import jax.numpy as jnp
from jax import lax
from jax.experimental import pallas as pl
from jax.experimental.pallas import tpu as pltpu
from jax.sharding import PartitionSpec as P

gate_scale = 8.0
input_eps = 1e-06
head_eps = 1e-05
f32 = jnp.float32
bf16 = jnp.bfloat16
MESH = pl.DeviceIdType.MESH
HALO = 16


def softplus(x):
    u = jnp.exp(-jnp.abs(x))
    z = u / (2.0 + u)
    zz = z * z
    series = jnp.zeros_like(z)
    for power in range(17, 0, -2):
        series = series * zz + 1.0 / power
    return jnp.maximum(x, 0.0) + 2.0 * z * series


def neg_expm1(y, exp_y):
    series = jnp.ones_like(y)
    for k in range(8, 1, -1):
        series = 1.0 + series * y * (1.0 / k)
    return jnp.where(y > -0.25, -y * series, 1.0 - exp_y)


def shifted(x, k, fill):
    if k % 8 == 0:
        return jnp.concatenate([jnp.full((k, x.shape[1]), fill, x.dtype), x[:-k]], axis=0)
    row = lax.broadcasted_iota(jnp.int32, x.shape, 0)
    return jnp.where(row < k, fill, pltpu.roll(x, k, 0))


def kernel(
    sizes,
    tokens, norm_gain, query_weight, w_key, w_value, w_input, w_gate, conv_kernel, w_recur, w_admit,
    decay_param, decay_scale, init_state, diff_lambda, head_gain, w_out_lru, w_out_attn,
    out,
    tok, normed, w_all, w_out, conv_v, recur_v, admit_v, chan_v, scale_v, hg_v, ng_v,
    kv, ext, halo_src, halo_dst, stat, qs, peak, total, acc, mix, send_a, recv_a, own, send_b, recv_b,
    local_sem, tok_send, tok_recv, fwd_send, fwd_recv, kv_send, kv_recv, halo_sem, stat_send, stat_recv,
    a_send, a_recv, b_send, b_recv, near_send, near_recv,
):
    n_s, n_f, n_t = sizes
    assert n_f == 4
    s, f, t = (lax.axis_index(a) for a in ("sp", "fs", "tp"))
    group = n_f * n_t
    rows = tokens.shape[0]
    span = rows * group
    chans = w_input.shape[1]
    width = query_weight.shape[1]
    kw = w_key.shape[1]
    vw = w_value.shape[1]
    me = f * n_t + t

    here = [
        (tokens, tok.at[me]),
        (norm_gain, ng_v),
        (w_key, w_all.at[:, pl.ds(0, kw)]),
        (w_value, w_all.at[:, pl.ds(kw, vw)]),
        (w_input, w_all.at[:, pl.ds(kw + vw, chans)]),
        (w_gate, w_all.at[:, pl.ds(kw + vw + chans, chans)]),
        (query_weight, w_all.at[:, pl.ds(kw + vw + 2 * chans, width)]),
        (conv_kernel, conv_v),
        (w_recur, recur_v),
        (w_admit, admit_v),
        (decay_param, chan_v.at[0]),
        (init_state, chan_v.at[1]),
        (decay_scale, scale_v),
        (head_gain, hg_v),
        (w_out_lru, w_out.at[pl.ds(0, chans)]),
        (w_out_attn, w_out.at[pl.ds(chans, w_out_attn.shape[0])]),
    ]
    here = [pltpu.make_async_copy(a, b, local_sem.at[i]) for i, (a, b) in enumerate(here)]
    for copy in here:
        copy.start()

    barrier = pltpu.get_barrier_semaphore()
    for df in range(n_f):
        for dt in range(n_t):
            if df or dt:
                pl.semaphore_signal(
                    barrier, inc=1, device_id_type=MESH,
                    device_id={"fs": lax.rem(f + df, n_f), "tp": lax.rem(t + dt, n_t)},
                )

    def greet(k, c):
        pl.semaphore_signal(barrier, inc=1, device_id={"sp": lax.rem(s + k, n_s)}, device_id_type=MESH)
        return c

    lax.fori_loop(1, n_s, greet, 0)
    pl.semaphore_wait(barrier, group - 1 + n_s - 1)

    def remote(src, dst, ss, rs, **where):
        return pltpu.make_async_remote_copy(
            src_ref=src, dst_ref=dst, send_sem=ss, recv_sem=rs, device_id=where, device_id_type=MESH
        )

    here[0].wait()
    here[1].wait()
    sends = []
    half = rows // 2
    near = f + 1 - 2 * lax.rem(f, 2)
    far = lax.rem(f + n_f // 2, n_f)
    diagonal = lax.rem(near + n_f // 2, n_f)

    def part(owner, core, h):
        return tok.at[owner * n_t + core, pl.ds(h * half, half)]

    def gather(owner, h, slot, target):
        copy = remote(part(owner, t, h), part(owner, t, h), tok_send.at[slot], tok_recv.at[slot], fs=target)
        copy.start()
        sends.append(copy)

    gather(f, 0, 0, near)
    gather(f, 1, 3, far)
    gather(f, 1, 1, near)
    gather(f, 0, 2, far)

    def arrived(owner, h, slot):
        remote(part(owner, t, h), part(owner, t, h), tok_send.at[slot], tok_recv.at[slot], fs=f).wait_recv()
        if slot == 0:
            gather(owner, h, 4, far)
        if slot == 3:
            gather(owner, h, 5, near)
        forward(owner, h, slot)

    def forward(owner, h, slot):
        for dt in range(1, n_t):
            copy = remote(
                part(owner, t, h), part(owner, t, h), fwd_send.at[slot, dt], fwd_recv.at[slot, dt],
                tp=lax.rem(t + dt, n_t),
            )
            copy.start()
            sends.append(copy)

    def partner(owner, first_slot):
        for dt in range(1, n_t):
            core = lax.rem(t + n_t - dt, n_t)
            for h in range(2):
                slot = first_slot + h
                remote(
                    part(owner, core, h), part(owner, core, h), fwd_send.at[slot, dt], fwd_recv.at[slot, dt], tp=t
                ).wait_recv()
            normalize(owner * n_t + core)

    def normalize(slot):
        x = tok[slot].astype(f32)
        x = x * lax.rsqrt(jnp.mean(x * x, axis=1, keepdims=True) + input_eps) * ng_v[...]
        normed[pl.ds(pl.multiple_of(slot * rows, rows), rows), :] = x.astype(bf16)

    forward(f, 0, 6)
    forward(f, 1, 7)
    normalize(me)
    partner(f, 6)
    arrived(near, 0, 0)
    arrived(far, 1, 3)
    arrived(near, 1, 1)
    arrived(far, 0, 2)
    normalize(near * n_t + t)
    normalize(far * n_t + t)
    partner(near, 0)
    partner(far, 2)
    arrived(diagonal, 0, 4)
    arrived(diagonal, 1, 5)
    normalize(diagonal * n_t + t)
    partner(diagonal, 4)

    for copy in here[2:]:
        copy.wait()
    x = normed[...]
    kv[s] = jnp.dot(x, w_all[:, : kw + vw], preferred_element_type=f32).astype(bf16)
    piece_rows = span // n_f
    mine = pl.ds(pl.multiple_of(f * piece_rows, piece_rows), piece_rows)

    def send_kv(k, c):
        k = later + 1 - k
        remote(kv.at[s, mine], kv.at[s, mine], kv_send.at[k], kv_recv.at[s], sp=s + k).start()
        return c

    later = n_s - 1 - s
    rest = jnp.dot(x, w_all[:, kw + vw :], preferred_element_type=f32).astype(bf16)
    lru_in = rest[:, :chans]
    halo_src[...] = lru_in[span - HALO :]
    lax.fori_loop(1, later + 1, send_kv, 0)
    halo_copy = remote(halo_src, halo_dst, halo_sem.at[0], halo_sem.at[1], sp=lax.rem(s + 1, n_s))

    @pl.when(s + 1 < n_s)
    def _():
        halo_copy.start()

    gate_proj = rest[:, chans : 2 * chans].astype(f32)
    gate = 0.5 * gate_proj * (
        1.0 + jnp.tanh(0.7978845608028654 * (gate_proj + 0.044715 * gate_proj * gate_proj * gate_proj))
    )
    q = rest[:, 2 * chans :]
    size_qk = width // 2
    first = lax.broadcasted_iota(jnp.int32, (span, width), 1) < size_qk
    zero = jnp.zeros_like(q)
    qs[pl.ds(0, span), :] = jnp.where(first, q, zero)
    qs[pl.ds(span, span), :] = jnp.where(first, zero, q)
    score_scale = size_qk ** (-0.5)

    def scores_of(j):
        return lax.dot_general(
            qs[...], kv[j, :, pl.ds(0, kw)], (((1,), (1,)), ((), ())), preferred_element_type=f32
        ) * score_scale

    ext[pl.ds(HALO, span), :] = lru_in.astype(f32)

    @pl.when(s == 0)
    def _():
        ext[pl.ds(0, HALO), :] = jnp.zeros((HALO, chans), f32)

    @pl.when(s > 0)
    def _():
        halo_copy.wait_recv()
        ext[pl.ds(0, HALO), :] = halo_dst[...].astype(f32)

    taps = conv_kernel.shape[0]
    conv = jnp.zeros((span, chans), f32)
    for j in range(taps):
        conv = conv + conv_v[pl.ds(j, 1), :] * ext[pl.ds(HALO - taps + 1 + j, span), :]
    conv = conv.astype(bf16)
    blocks, bd = w_recur.shape[0], w_recur.shape[1]
    lines = []
    for n in range(blocks):
        parts = []
        for ref in (recur_v, admit_v):
            for m in range(blocks):
                parts.append(ref[n] if m == n else jnp.zeros((bd, bd), bf16))
        lines.append(jnp.concatenate(parts, axis=1))
    gates = jax.nn.sigmoid(jnp.dot(conv, jnp.concatenate(lines, axis=0), preferred_element_type=f32))
    log_decay = -gate_scale * gates[:, :chans] * softplus(-chan_v[0]) * scale_v[...]
    a = jnp.exp(log_decay)
    b = jnp.sqrt(neg_expm1(2.0 * log_decay, a * a)) * gates[:, chans:] * conv.astype(f32)
    k = 1
    while k < span:
        b = a * shifted(b, k, 0.0) + b
        a = a * shifted(a, k, 1.0)
        k *= 2
    stat[s, pl.ds(0, 8), :] = jnp.broadcast_to(a[span - 1 :], (8, chans))
    stat[s, pl.ds(8, 8), :] = jnp.broadcast_to(b[span - 1 :], (8, chans))

    def send_stat(k, c):
        k = later + 1 - k
        remote(stat.at[s], stat.at[s], stat_send.at[k], stat_recv.at[s], sp=s + k).start()
        return c

    lax.fori_loop(1, later + 1, send_stat, 0)

    def spread(df, j):
        return remote(
            kv.at[j, mine], kv.at[j, mine], near_send.at[j, df], near_recv.at[j, df],
            fs=(f, diagonal, near, far)[df],
        )

    def pass_on(k, c):
        j = s - 1 - k
        remote(kv.at[j, mine], kv.at[j, mine], kv_send.at[0], kv_recv.at[j], sp=s).wait_recv()
        for df in range(1, n_f):
            spread(df, j).start()
        return c

    lax.fori_loop(0, jnp.minimum(s, 1), pass_on, 0)

    sc = scores_of(s)
    row = lax.broadcasted_iota(jnp.int32, (span, span), 0)
    col = lax.broadcasted_iota(jnp.int32, (span, span), 1)
    see = jnp.concatenate([col <= row, col <= row], axis=0)
    sc = jnp.where(see, sc, -1e30)
    top = jnp.max(sc, axis=1, keepdims=True)
    p = jnp.where(see, jnp.exp(sc - top), 0.0)

    peak[...] = top
    total[...] = jnp.sum(p, axis=1, keepdims=True)
    acc[...] = jnp.dot(p.astype(bf16), kv[s, :, pl.ds(kw, vw)], preferred_element_type=f32)

    lax.fori_loop(1, s, pass_on, 0)

    def earlier_keys(k, c):
        j = s - 1 - k
        for df in range(1, n_f):
            theirs = (f, diagonal, near, far)[df] * piece_rows
            theirs = pl.ds(pl.multiple_of(theirs, piece_rows), piece_rows)
            remote(kv.at[j, theirs], kv.at[j, theirs], near_send.at[j, df], near_recv.at[j, df], fs=f).wait_recv()
        sc = scores_of(j)
        old = peak[...]
        top = jnp.maximum(old, jnp.max(sc, axis=1, keepdims=True))
        p = jnp.exp(sc - top)
        fade = jnp.exp(old - top)
        peak[...] = top
        total[...] = total[...] * fade + jnp.sum(p, axis=1, keepdims=True)
        acc[...] = acc[...] * fade + jnp.dot(p.astype(bf16), kv[j, :, pl.ds(kw, vw)], preferred_element_type=f32)
        return c

    lax.fori_loop(0, s, earlier_keys, 0)
    def enter(k, state):
        remote(stat.at[k], stat.at[k], stat_send.at[0], stat_recv.at[k], sp=s).wait_recv()
        return stat[k, pl.ds(0, 1), :] * state + stat[k, pl.ds(8, 1), :]

    entering = lax.fori_loop(0, s, enter, chan_v[1])
    lru_out = ((b + a * entering) * gate).astype(bf16)
    mix[:, :, :, pl.ds(0, chans)] = lru_out.reshape(n_f, n_t, rows, chans)

    heads = acc[...] / total[...]
    diff = heads[:span] - diff_lambda[0] * heads[span:]
    scaled = diff * lax.rsqrt(jnp.mean(diff * diff, axis=1, keepdims=True) + head_eps) * hg_v[...]
    mix[:, :, :, pl.ds(chans, vw)] = scaled.astype(bf16).reshape(n_f, n_t, rows, vw)

    depth = chans + vw
    order = (diagonal, near, far, f)
    cut = out.shape[1] // 2

    def reduce(slot, target, value):
        send_b[slot] = value.astype(bf16)
        copy = remote(send_b.at[slot], recv_b.at[slot], b_send.at[slot], b_recv.at[slot], fs=target)
        copy.start()
        sends.append(copy)

    def taken(slot):
        remote(send_b.at[slot], recv_b.at[slot], b_send.at[slot], b_recv.at[slot], fs=f).wait_recv()
        return recv_b[slot].astype(f32)

    for dt in range(1, n_t):
        there = lax.rem(t + dt, n_t)
        share = jnp.dot(mix[:, there].reshape(n_f * rows, depth), w_out[...], preferred_element_type=f32)
        send_a[dt - 1] = share.astype(bf16).reshape(n_f, rows, share.shape[1])
        for i, g in enumerate(order):
            copy = remote(
                send_a.at[dt - 1, g], recv_a.at[dt - 1, g], a_send.at[dt - 1, i], a_recv.at[dt - 1, i], tp=there
            )
            copy.start()
            sends.append(copy)
    share = jnp.dot(mix[:, t].reshape(n_f * rows, depth), w_out[...], preferred_element_type=f32)
    own[...] = share.reshape(own.shape)
    for i, g in enumerate(order):
        for dt in range(1, n_t):
            remote(
                send_a.at[dt - 1, g], recv_a.at[dt - 1, g], a_send.at[dt - 1, i], a_recv.at[dt - 1, i], tp=t
            ).wait_recv()
            own[g] += recv_a[dt - 1, g].astype(f32)
        if g is diagonal:
            reduce(0, near, own[g, :, :cut])
            reduce(1, far, own[g, :, cut:])
        if g is near:
            reduce(2, near, own[g, :, :cut])
        if g is far:
            reduce(3, far, own[g, :, cut:])
    reduce(4, far, own[far, :, :cut] + taken(0))
    reduce(5, near, own[near, :, cut:] + taken(1))
    left = own[f, :, :cut] + taken(2)
    right = own[f, :, cut:] + taken(3)
    out[:, :cut] = (left + taken(4)).astype(bf16)
    out[:, cut:] = (right + taken(5)).astype(bf16)

    for copy in sends:
        copy.wait_send()

    @pl.when(s + 1 < n_s)
    def _():
        halo_copy.wait_send()

    def drain(k, c):
        remote(kv.at[s, mine], kv.at[s, mine], kv_send.at[k], kv_recv.at[s], sp=s + k).wait_send()
        remote(stat.at[s], stat.at[s], stat_send.at[k], stat_recv.at[s], sp=s + k).wait_send()
        return c

    lax.fori_loop(1, later + 1, drain, 0)

    def drain_near(j, c):
        for df in range(1, n_f):
            spread(df, j).wait_send()
        return c

    lax.fori_loop(0, s, drain_near, 0)


def body(sizes, *args):
    n_s, n_f, n_t = sizes
    (tokens, norm_gain, query_weight, w_key, w_value, w_input, w_gate, conv_kernel, w_recur, w_admit,
     decay_param, decay_scale, init_state, diff_lambda, head_gain, w_out_lru, w_out_attn) = args
    rows, d = tokens.shape
    group = n_f * n_t
    span = rows * group
    chans = w_input.shape[1]
    kw, vw, width = w_key.shape[1], w_value.shape[1], query_weight.shape[1]
    operands = (
        tokens, norm_gain[None], query_weight, w_key, w_value, w_input, w_gate, conv_kernel, w_recur, w_admit,
        decay_param[None], decay_scale, init_state[None], diff_lambda, head_gain[None], w_out_lru, w_out_attn,
    )
    dma = pltpu.SemaphoreType.DMA
    scratch = [
        pltpu.VMEM((group, rows, d), bf16),
        pltpu.VMEM((span, d), bf16),
        pltpu.VMEM((d, kw + vw + 2 * chans + width), bf16),
        pltpu.VMEM((chans + vw, d), bf16),
        pltpu.VMEM(conv_kernel.shape, f32),
        pltpu.VMEM(w_recur.shape, bf16),
        pltpu.VMEM(w_admit.shape, bf16),
        pltpu.VMEM((2, 1, chans), f32),
        pltpu.VMEM((span, chans), f32),
        pltpu.VMEM((1, vw), f32),
        pltpu.VMEM((1, d), f32),
        pltpu.VMEM((n_s, span, kw + vw), bf16),
        pltpu.VMEM((span + HALO, chans), f32),
        pltpu.VMEM((HALO, chans), bf16),
        pltpu.VMEM((HALO, chans), bf16),
        pltpu.VMEM((n_s, 16, chans), f32),
        pltpu.VMEM((2 * span, width), bf16),
        pltpu.VMEM((2 * span, 1), f32),
        pltpu.VMEM((2 * span, 1), f32),
        pltpu.VMEM((2 * span, vw), f32),
        pltpu.VMEM((n_f, n_t, rows, chans + vw), bf16),
        pltpu.VMEM((n_t - 1, n_f, rows, d), bf16),
        pltpu.VMEM((n_t - 1, n_f, rows, d), bf16),
        pltpu.VMEM((n_f, rows, d), f32),
        pltpu.VMEM((6, rows, d // 2), bf16),
        pltpu.VMEM((6, rows, d // 2), bf16),
        dma((len(operands),)),
        dma((6,)),
        dma((6,)),
        dma((8, n_t)),
        dma((8, n_t)),
        dma((n_s,)),
        dma((n_s,)),
        dma((2,)),
        dma((n_s,)),
        dma((n_s,)),
        dma((n_t - 1, n_f)),
        dma((n_t - 1, n_f)),
        dma((6,)),
        dma((6,)),
        dma((n_s, n_f)),
        dma((n_s, n_f)),
    ]
    return pl.pallas_call(
        functools.partial(kernel, sizes),
        out_shape=jax.ShapeDtypeStruct((rows, d), bf16),
        in_specs=[pl.BlockSpec(memory_space=pltpu.SMEM if a is diff_lambda else pl.ANY) for a in operands],
        out_specs=pl.BlockSpec(memory_space=pltpu.VMEM),
        scratch_shapes=scratch,
        compiler_params=pltpu.CompilerParams(
            collective_id=0, has_side_effects=True, vmem_limit_bytes=67043328
        ),
    )(*operands)


def solution(mesh):
    sizes = tuple(mesh.shape[a] for a in ("sp", "fs", "tp"))
    placed = (
        P(("sp", "fs", "tp"), None),
        P(),
        P(None, ("fs", "tp")),
        P(None, "tp"),
        P(None, "tp"),
        P(None, ("fs", "tp")),
        P(None, ("fs", "tp")),
        P(None, ("fs", "tp")),
        P(("fs", "tp"), None, None),
        P(("fs", "tp"), None, None),
        P(("fs", "tp")),
        P("sp", ("fs", "tp")),
        P(("fs", "tp")),
        P(("fs", "tp")),
        P(),
        P(("fs", "tp"), None),
        P(("fs", "tp"), None),
    )
    return jax.shard_map(
        functools.partial(body, sizes), mesh=mesh, in_specs=placed, out_specs=P(("sp", "fs", "tp"), None), check_vma=False
    )
```

```python
import functools

import jax
import jax.numpy as jnp
from jax import lax
from jax.experimental import pallas as pl
from jax.experimental.pallas import tpu as pltpu
from jax.sharding import PartitionSpec as P

gate_scale = 8.0
input_eps = 1e-06
head_eps = 1e-05
f32 = jnp.float32
bf16 = jnp.bfloat16
MESH = pl.DeviceIdType.MESH
HALO = 16


def softplus(x):
    u = jnp.exp(-jnp.abs(x))
    z = u / (2.0 + u)
    zz = z * z
    series = jnp.zeros_like(z)
    for power in range(17, 0, -2):
        series = series * zz + 1.0 / power
    return jnp.maximum(x, 0.0) + 2.0 * z * series


def neg_expm1(y, exp_y):
    series = jnp.ones_like(y)
    for k in range(8, 1, -1):
        series = 1.0 + series * y * (1.0 / k)
    return jnp.where(y > -0.25, -y * series, 1.0 - exp_y)


def shifted(x, k, fill):
    if k % 8 == 0:
        return jnp.concatenate([jnp.full((k, x.shape[1]), fill, x.dtype), x[:-k]], axis=0)
    row = lax.broadcasted_iota(jnp.int32, x.shape, 0)
    return jnp.where(row < k, fill, pltpu.roll(x, k, 0))


def kernel(
    sizes,
    tokens, norm_gain, query_weight, w_key, w_value, w_input, w_gate, conv_kernel, w_recur, w_admit,
    decay_param, decay_scale, init_state, diff_lambda, head_gain, w_out_lru, w_out_attn,
    out,
    tok, normed, w_all, w_out, conv_v, recur_v, admit_v, chan_v, scale_v, hg_v, ng_v,
    kv, ext, halo_src, halo_dst, stat, qs, peak, total, acc, mix, send_a, recv_a, own, send_b, recv_b,
    local_sem, tok_send, tok_recv, fwd_send, fwd_recv, kv_send, kv_recv, halo_sem, stat_send, stat_recv,
    a_send, a_recv, b_send, b_recv, near_send, near_recv,
):
    n_s, n_f, n_t = sizes
    assert n_f == 4
    s, f, t = (lax.axis_index(a) for a in ("sp", "fs", "tp"))
    group = n_f * n_t
    rows = tokens.shape[0]
    span = rows * group
    chans = w_input.shape[1]
    width = query_weight.shape[1]
    kw = w_key.shape[1]
    vw = w_value.shape[1]
    me = f * n_t + t

    here = [
        (tokens, tok.at[me]),
        (norm_gain, ng_v),
        (w_key, w_all.at[:, pl.ds(0, kw)]),
        (w_value, w_all.at[:, pl.ds(kw, vw)]),
        (w_input, w_all.at[:, pl.ds(kw + vw, chans)]),
        (w_gate, w_all.at[:, pl.ds(kw + vw + chans, chans)]),
        (query_weight, w_all.at[:, pl.ds(kw + vw + 2 * chans, width)]),
        (conv_kernel, conv_v),
        (w_recur, recur_v),
        (w_admit, admit_v),
        (decay_param, chan_v.at[0]),
        (init_state, chan_v.at[1]),
        (decay_scale, scale_v),
        (head_gain, hg_v),
        (w_out_lru, w_out.at[pl.ds(0, chans)]),
        (w_out_attn, w_out.at[pl.ds(chans, w_out_attn.shape[0])]),
    ]
    here = [pltpu.make_async_copy(a, b, local_sem.at[i]) for i, (a, b) in enumerate(here)]
    for copy in here:
        copy.start()

    barrier = pltpu.get_barrier_semaphore()
    for df in range(n_f):
        for dt in range(n_t):
            if df or dt:
                pl.semaphore_signal(
                    barrier, inc=1, device_id_type=MESH,
                    device_id={"fs": lax.rem(f + df, n_f), "tp": lax.rem(t + dt, n_t)},
                )

    def greet(k, c):
        pl.semaphore_signal(barrier, inc=1, device_id={"sp": lax.rem(s + k, n_s)}, device_id_type=MESH)
        return c

    lax.fori_loop(1, n_s, greet, 0)
    pl.semaphore_wait(barrier, group - 1 + n_s - 1)

    def remote(src, dst, ss, rs, **where):
        return pltpu.make_async_remote_copy(
            src_ref=src, dst_ref=dst, send_sem=ss, recv_sem=rs, device_id=where, device_id_type=MESH
        )

    here[0].wait()
    here[1].wait()
    sends = []
    half = rows // 2
    near = f + 1 - 2 * lax.rem(f, 2)
    far = lax.rem(f + n_f // 2, n_f)
    diagonal = lax.rem(near + n_f // 2, n_f)

    def part(owner, core, h):
        return tok.at[owner * n_t + core, pl.ds(h * half, half)]

    def gather(owner, h, slot, target):
        copy = remote(part(owner, t, h), part(owner, t, h), tok_send.at[slot], tok_recv.at[slot], fs=target)
        copy.start()
        sends.append(copy)

    gather(f, 0, 0, near)
    gather(f, 1, 3, far)
    gather(f, 1, 1, near)
    gather(f, 0, 2, far)

    def arrived(owner, h, slot):
        remote(part(owner, t, h), part(owner, t, h), tok_send.at[slot], tok_recv.at[slot], fs=f).wait_recv()
        if slot == 0:
            gather(owner, h, 4, far)
        if slot == 3:
            gather(owner, h, 5, near)
        forward(owner, h, slot)

    def forward(owner, h, slot):
        for dt in range(1, n_t):
            copy = remote(
                part(owner, t, h), part(owner, t, h), fwd_send.at[slot, dt], fwd_recv.at[slot, dt],
                tp=lax.rem(t + dt, n_t),
            )
            copy.start()
            sends.append(copy)

    def partner(owner, first_slot):
        for dt in range(1, n_t):
            core = lax.rem(t + n_t - dt, n_t)
            for h in range(2):
                slot = first_slot + h
                remote(
                    part(owner, core, h), part(owner, core, h), fwd_send.at[slot, dt], fwd_recv.at[slot, dt], tp=t
                ).wait_recv()
            normalize(owner * n_t + core)

    def normalize(slot):
        x = tok[slot].astype(f32)
        x = x * lax.rsqrt(jnp.mean(x * x, axis=1, keepdims=True) + input_eps) * ng_v[...]
        normed[pl.ds(pl.multiple_of(slot * rows, rows), rows), :] = x.astype(bf16)

    forward(f, 0, 6)
    forward(f, 1, 7)
    normalize(me)
    partner(f, 6)
    arrived(near, 0, 0)
    arrived(far, 1, 3)
    arrived(near, 1, 1)
    arrived(far, 0, 2)
    normalize(near * n_t + t)
    normalize(far * n_t + t)
    partner(near, 0)
    partner(far, 2)
    arrived(diagonal, 0, 4)
    arrived(diagonal, 1, 5)
    normalize(diagonal * n_t + t)
    partner(diagonal, 4)

    for copy in here[2:]:
        copy.wait()
    x = normed[...]
    kv[s] = jnp.dot(x, w_all[:, : kw + vw], preferred_element_type=f32).astype(bf16)
    piece_rows = span // n_f
    mine = pl.ds(pl.multiple_of(f * piece_rows, piece_rows), piece_rows)

    def send_kv(k, c):
        remote(kv.at[s, mine], kv.at[s, mine], kv_send.at[k], kv_recv.at[s], sp=s + k).start()
        return c

    later = n_s - 1 - s
    rest = jnp.dot(x, w_all[:, kw + vw :], preferred_element_type=f32).astype(bf16)
    lru_in = rest[:, :chans]
    halo_src[...] = lru_in[span - HALO :]
    lax.fori_loop(1, later + 1, send_kv, 0)
    halo_copy = remote(halo_src, halo_dst, halo_sem.at[0], halo_sem.at[1], sp=lax.rem(s + 1, n_s))

    @pl.when(s + 1 < n_s)
    def _():
        halo_copy.start()

    gate_proj = rest[:, chans : 2 * chans].astype(f32)
    gate = 0.5 * gate_proj * (
        1.0 + jnp.tanh(0.7978845608028654 * (gate_proj + 0.044715 * gate_proj * gate_proj * gate_proj))
    )
    q = rest[:, 2 * chans :]
    size_qk = width // 2
    first = lax.broadcasted_iota(jnp.int32, (span, width), 1) < size_qk
    zero = jnp.zeros_like(q)
    qs[pl.ds(0, span), :] = jnp.where(first, q, zero)
    qs[pl.ds(span, span), :] = jnp.where(first, zero, q)
    score_scale = size_qk ** (-0.5)

    def scores_of(j):
        return lax.dot_general(
            qs[...], kv[j, :, pl.ds(0, kw)], (((1,), (1,)), ((), ())), preferred_element_type=f32
        ) * score_scale

    ext[pl.ds(HALO, span), :] = lru_in.astype(f32)

    @pl.when(s == 0)
    def _():
        ext[pl.ds(0, HALO), :] = jnp.zeros((HALO, chans), f32)

    @pl.when(s > 0)
    def _():
        halo_copy.wait_recv()
        ext[pl.ds(0, HALO), :] = halo_dst[...].astype(f32)

    taps = conv_kernel.shape[0]
    conv = jnp.zeros((span, chans), f32)
    for j in range(taps):
        conv = conv + conv_v[pl.ds(j, 1), :] * ext[pl.ds(HALO - taps + 1 + j, span), :]
    conv = conv.astype(bf16)
    blocks, bd = w_recur.shape[0], w_recur.shape[1]
    lines = []
    for n in range(blocks):
        parts = []
        for ref in (recur_v, admit_v):
            for m in range(blocks):
                parts.append(ref[n] if m == n else jnp.zeros((bd, bd), bf16))
        lines.append(jnp.concatenate(parts, axis=1))
    gates = jax.nn.sigmoid(jnp.dot(conv, jnp.concatenate(lines, axis=0), preferred_element_type=f32))
    log_decay = -gate_scale * gates[:, :chans] * softplus(-chan_v[0]) * scale_v[...]
    a = jnp.exp(log_decay)
    b = jnp.sqrt(neg_expm1(2.0 * log_decay, a * a)) * gates[:, chans:] * conv.astype(f32)
    k = 1
    while k < span:
        b = a * shifted(b, k, 0.0) + b
        a = a * shifted(a, k, 1.0)
        k *= 2
    stat[s, pl.ds(0, 8), :] = jnp.broadcast_to(a[span - 1 :], (8, chans))
    stat[s, pl.ds(8, 8), :] = jnp.broadcast_to(b[span - 1 :], (8, chans))

    def send_stat(k, c):
        remote(stat.at[s], stat.at[s], stat_send.at[k], stat_recv.at[s], sp=s + k).start()
        return c

    lax.fori_loop(1, later + 1, send_stat, 0)

    def spread(df, j):
        return remote(
            kv.at[j, mine], kv.at[j, mine], near_send.at[j, df], near_recv.at[j, df], fs=lax.rem(f + df, n_f)
        )

    def pass_on(k, c):
        j = s - 1 - k
        remote(kv.at[j, mine], kv.at[j, mine], kv_send.at[0], kv_recv.at[j], sp=s).wait_recv()
        for df in range(1, n_f):
            spread(df, j).start()
        return c

    lax.fori_loop(0, jnp.minimum(s, 1), pass_on, 0)

    sc = scores_of(s)
    row = lax.broadcasted_iota(jnp.int32, (span, span), 0)
    col = lax.broadcasted_iota(jnp.int32, (span, span), 1)
    see = jnp.concatenate([col <= row, col <= row], axis=0)
    sc = jnp.where(see, sc, -1e30)
    top = jnp.max(sc, axis=1, keepdims=True)
    p = jnp.where(see, jnp.exp(sc - top), 0.0)

    peak[...] = top
    total[...] = jnp.sum(p, axis=1, keepdims=True)
    acc[...] = jnp.dot(p.astype(bf16), kv[s, :, pl.ds(kw, vw)], preferred_element_type=f32)

    lax.fori_loop(1, s, pass_on, 0)

    def earlier_keys(k, c):
        j = s - 1 - k
        for df in range(1, n_f):
            theirs = lax.rem(f + n_f - df, n_f) * piece_rows
            theirs = pl.ds(pl.multiple_of(theirs, piece_rows), piece_rows)
            remote(kv.at[j, theirs], kv.at[j, theirs], near_send.at[j, df], near_recv.at[j, df], fs=f).wait_recv()
        sc = scores_of(j)
        old = peak[...]
        top = jnp.maximum(old, jnp.max(sc, axis=1, keepdims=True))
        p = jnp.exp(sc - top)
        fade = jnp.exp(old - top)
        peak[...] = top
        total[...] = total[...] * fade + jnp.sum(p, axis=1, keepdims=True)
        acc[...] = acc[...] * fade + jnp.dot(p.astype(bf16), kv[j, :, pl.ds(kw, vw)], preferred_element_type=f32)
        return c

    lax.fori_loop(0, s, earlier_keys, 0)
    def enter(k, state):
        remote(stat.at[k], stat.at[k], stat_send.at[0], stat_recv.at[k], sp=s).wait_recv()
        return stat[k, pl.ds(0, 1), :] * state + stat[k, pl.ds(8, 1), :]

    entering = lax.fori_loop(0, s, enter, chan_v[1])
    lru_out = ((b + a * entering) * gate).astype(bf16)
    mix[:, :, :, pl.ds(0, chans)] = lru_out.reshape(n_f, n_t, rows, chans)

    heads = acc[...] / total[...]
    diff = heads[:span] - diff_lambda[0] * heads[span:]
    scaled = diff * lax.rsqrt(jnp.mean(diff * diff, axis=1, keepdims=True) + head_eps) * hg_v[...]
    mix[:, :, :, pl.ds(chans, vw)] = scaled.astype(bf16).reshape(n_f, n_t, rows, vw)

    depth = chans + vw
    order = (diagonal, near, far, f)
    cut = out.shape[1] // 2

    def reduce(slot, target, value):
        send_b[slot] = value.astype(bf16)
        copy = remote(send_b.at[slot], recv_b.at[slot], b_send.at[slot], b_recv.at[slot], fs=target)
        copy.start()
        sends.append(copy)

    def taken(slot):
        remote(send_b.at[slot], recv_b.at[slot], b_send.at[slot], b_recv.at[slot], fs=f).wait_recv()
        return recv_b[slot].astype(f32)

    for dt in range(1, n_t):
        there = lax.rem(t + dt, n_t)
        share = jnp.dot(mix[:, there].reshape(n_f * rows, depth), w_out[...], preferred_element_type=f32)
        send_a[dt - 1] = share.astype(bf16).reshape(n_f, rows, share.shape[1])
        for i, g in enumerate(order):
            copy = remote(
                send_a.at[dt - 1, g], recv_a.at[dt - 1, g], a_send.at[dt - 1, i], a_recv.at[dt - 1, i], tp=there
            )
            copy.start()
            sends.append(copy)
    share = jnp.dot(mix[:, t].reshape(n_f * rows, depth), w_out[...], preferred_element_type=f32)
    own[...] = share.reshape(own.shape)
    for i, g in enumerate(order):
        for dt in range(1, n_t):
            remote(
                send_a.at[dt - 1, g], recv_a.at[dt - 1, g], a_send.at[dt - 1, i], a_recv.at[dt - 1, i], tp=t
            ).wait_recv()
            own[g] += recv_a[dt - 1, g].astype(f32)
        if g is diagonal:
            reduce(0, near, own[g, :, :cut])
            reduce(1, far, own[g, :, cut:])
        if g is near:
            reduce(2, near, own[g, :, :cut])
        if g is far:
            reduce(3, far, own[g, :, cut:])
    reduce(4, far, own[far, :, :cut] + taken(0))
    reduce(5, near, own[near, :, cut:] + taken(1))
    left = own[f, :, :cut] + taken(2)
    right = own[f, :, cut:] + taken(3)
    out[:, :cut] = (left + taken(4)).astype(bf16)
    out[:, cut:] = (right + taken(5)).astype(bf16)

    for copy in sends:
        copy.wait_send()

    @pl.when(s + 1 < n_s)
    def _():
        halo_copy.wait_send()

    def drain(k, c):
        remote(kv.at[s, mine], kv.at[s, mine], kv_send.at[k], kv_recv.at[s], sp=s + k).wait_send()
        remote(stat.at[s], stat.at[s], stat_send.at[k], stat_recv.at[s], sp=s + k).wait_send()
        return c

    lax.fori_loop(1, later + 1, drain, 0)

    def drain_near(j, c):
        for df in range(1, n_f):
            spread(df, j).wait_send()
        return c

    lax.fori_loop(0, s, drain_near, 0)


def body(sizes, *args):
    n_s, n_f, n_t = sizes
    (tokens, norm_gain, query_weight, w_key, w_value, w_input, w_gate, conv_kernel, w_recur, w_admit,
     decay_param, decay_scale, init_state, diff_lambda, head_gain, w_out_lru, w_out_attn) = args
    rows, d = tokens.shape
    group = n_f * n_t
    span = rows * group
    chans = w_input.shape[1]
    kw, vw, width = w_key.shape[1], w_value.shape[1], query_weight.shape[1]
    operands = (
        tokens, norm_gain[None], query_weight, w_key, w_value, w_input, w_gate, conv_kernel, w_recur, w_admit,
        decay_param[None], decay_scale, init_state[None], diff_lambda, head_gain[None], w_out_lru, w_out_attn,
    )
    dma = pltpu.SemaphoreType.DMA
    scratch = [
        pltpu.VMEM((group, rows, d), bf16),
        pltpu.VMEM((span, d), bf16),
        pltpu.VMEM((d, kw + vw + 2 * chans + width), bf16),
        pltpu.VMEM((chans + vw, d), bf16),
        pltpu.VMEM(conv_kernel.shape, f32),
        pltpu.VMEM(w_recur.shape, bf16),
        pltpu.VMEM(w_admit.shape, bf16),
        pltpu.VMEM((2, 1, chans), f32),
        pltpu.VMEM((span, chans), f32),
        pltpu.VMEM((1, vw), f32),
        pltpu.VMEM((1, d), f32),
        pltpu.VMEM((n_s, span, kw + vw), bf16),
        pltpu.VMEM((span + HALO, chans), f32),
        pltpu.VMEM((HALO, chans), bf16),
        pltpu.VMEM((HALO, chans), bf16),
        pltpu.VMEM((n_s, 16, chans), f32),
        pltpu.VMEM((2 * span, width), bf16),
        pltpu.VMEM((2 * span, 1), f32),
        pltpu.VMEM((2 * span, 1), f32),
        pltpu.VMEM((2 * span, vw), f32),
        pltpu.VMEM((n_f, n_t, rows, chans + vw), bf16),
        pltpu.VMEM((n_t - 1, n_f, rows, d), bf16),
        pltpu.VMEM((n_t - 1, n_f, rows, d), bf16),
        pltpu.VMEM((n_f, rows, d), f32),
        pltpu.VMEM((6, rows, d // 2), bf16),
        pltpu.VMEM((6, rows, d // 2), bf16),
        dma((len(operands),)),
        dma((6,)),
        dma((6,)),
        dma((8, n_t)),
        dma((8, n_t)),
        dma((n_s,)),
        dma((n_s,)),
        dma((2,)),
        dma((n_s,)),
        dma((n_s,)),
        dma((n_t - 1, n_f)),
        dma((n_t - 1, n_f)),
        dma((6,)),
        dma((6,)),
        dma((n_s, n_f)),
        dma((n_s, n_f)),
    ]
    return pl.pallas_call(
        functools.partial(kernel, sizes),
        out_shape=pltpu.VMEM((rows, d), bf16),
        in_specs=[pl.BlockSpec(memory_space=pltpu.SMEM if a is diff_lambda else pl.ANY) for a in operands],
        out_specs=pl.BlockSpec(memory_space=pltpu.VMEM),
        scratch_shapes=scratch,
        compiler_params=pltpu.CompilerParams(
            collective_id=0, has_side_effects=True, vmem_limit_bytes=60000000
        ),
    )(*operands)


def solution(mesh):
    sizes = tuple(mesh.shape[a] for a in ("sp", "fs", "tp"))
    placed = (
        P(("sp", "fs", "tp"), None),
        P(),
        P(None, ("fs", "tp")),
        P(None, "tp"),
        P(None, "tp"),
        P(None, ("fs", "tp")),
        P(None, ("fs", "tp")),
        P(None, ("fs", "tp")),
        P(("fs", "tp"), None, None),
        P(("fs", "tp"), None, None),
        P(("fs", "tp")),
        P("sp", ("fs", "tp")),
        P(("fs", "tp")),
        P(("fs", "tp")),
        P(),
        P(("fs", "tp"), None),
        P(("fs", "tp"), None),
    )
    return jax.shard_map(
        functools.partial(body, sizes), mesh=mesh, in_specs=placed, out_specs=P(("sp", "fs", "tp"), None), check_vma=False
    )
```
